32 devices in a mesh: dp: 2 (over x), kv: 8 (over z, y), tp: 2 (over core).
Axes of the slice: x: 2, y: 2, z: 4, core: 2. Of those that a mesh axis runs over, the one named last changes fastest.
Arguments:
- tokens: bfloat16 [2, 1536, 2048], P('dp', 'kv'), may hold values from -60 to 60
- doc_lengths: int32 [2, 8], P('dp'), may hold values from 1 to 768, as said below
- picked: int32 [2, 48, 32], P('dp', 'kv'), may hold values from -1 to 47, as said below
- w_query: bfloat16 [2048, 1024], P(None, 'tp'), may hold values from -0.125 to 0.125
- w_key: bfloat16 [2048, 128], replicated, may hold values from -0.125 to 0.125
- w_value: bfloat16 [2048, 128], replicated, may hold values from -0.125 to 0.125
- w_out: bfloat16 [1024, 2048], replicated, may hold values from -0.1875 to 0.1875
Outputs:
- mixed: bfloat16 [2, 1536, 2048], P('dp', 'kv')
The draws below stay inside these ranges and needn't reach their ends.
Inputs may be any that keep to these rules, and one draw needn't show every extreme that they name: `doc_lengths`: each row sums to 1536; its largest document has exactly 768 positions. `picked`: slot 0 of query block b is b itself; the other slots hold distinct blocks before b, or -1 when fewer such blocks are named. Of the 6 blocks that one device of kv holds, at most 2 are named by query blocks held by other devices of kv, and in every row some device reaches 2.
All inputs are finite; a program needn't handle non-finite values.
Results may differ from the reference program's by a relative error of at most 0.011.
Values may be sent and summed in bfloat16 or wider, within the bound.
A program may use at most 64 MiB of HBM per device.

```python
import jax
import jax.numpy as jnp
from jax import lax

D = 2048
HEADS = 16
KV_HEADS = 2
HEAD_DIM = 64
BLOCK = 32
PICKS = 32
DOCS = 8
TOK_DEV = 192
GROUPS = 2
SEQ = 1536
NBLOCKS = 48


def pack_lengths(key):
    half = SEQ // 2

    def one_row(subkey):
        cuts = jnp.sort(jax.random.permutation(jax.random.fold_in(subkey, 1), half - 1)[:DOCS - 2].astype(jnp.int32) + 1)
        edges = jnp.concatenate([jnp.zeros((1,), jnp.int32), cuts, jnp.full((1,), half, jnp.int32)])
        small = edges[1:] - edges[:-1]
        place = jax.random.randint(jax.random.fold_in(subkey, 2), (), 0, DOCS)
        slot_ids = jnp.arange(DOCS, dtype=jnp.int32)
        before = jnp.concatenate([small, small[-1:]])
        after = jnp.concatenate([small[:1], small])
        return jnp.where(slot_ids < place, before, jnp.where(slot_ids == place, half, after)).astype(jnp.int32)
    subkeys = jax.random.split(jax.random.fold_in(key, 7), GROUPS)
    return jax.vmap(one_row)(subkeys)


def draw_doc_lengths(key, part):
    return pack_lengths(key)


def draw_picked(key, part):
    blocks_dev = TOK_DEV // BLOCK
    devices = NBLOCKS // blocks_dev
    midway = devices // 2

    def one_row(subkey):
        block_ids = jnp.arange(NBLOCKS, dtype=jnp.int32)
        owner = block_ids // blocks_dev
        within = block_ids % blocks_dev
        favored = jax.random.randint(jax.random.fold_in(subkey, 1), (devices,), 0, blocks_dev - 1).astype(jnp.int32)
        favored_block = favored[owner]
        hot_block = (within == blocks_dev - 1) | (within == favored_block)
        fame = jax.random.randint(jax.random.fold_in(subkey, 2), (devices,), 0, 4).astype(jnp.int32)[owner]
        base = jax.random.randint(jax.random.fold_in(subkey, 3), (NBLOCKS, NBLOCKS), 0, 1024).astype(jnp.int32)
        row_ids = block_ids[:, None]
        col_ids = block_ids[None, :]
        same_device = owner[:, None] == owner[None, :]
        allowed = (col_ids < row_ids) & (same_device | hot_block[None, :])
        previous = (col_ids == row_ids - 1).astype(jnp.int32) * 65536
        far_row = (owner[:, None] >= midway) & (within[:, None] == 0)
        far_col = (owner[None, :] == owner[:, None] - midway) & (within[None, :] == favored_block[None, :])
        far = (far_row & far_col).astype(jnp.int32) * 65536
        score = base + (fame * 1024)[None, :] + same_device.astype(jnp.int32) * 2048 + previous + far
        score = jnp.where(allowed, score * NBLOCKS + col_ids, -1)
        top_values, top_index = lax.top_k(score, PICKS - 1)
        others = jnp.where(top_values >= 0, top_index, -1)
        return jnp.concatenate([block_ids[:, None], others], axis=1).astype(jnp.int32)
    subkeys = jax.random.split(jax.random.fold_in(key, 11), GROUPS)
    return jax.vmap(one_row)(subkeys)


def draw_tokens(key, part):
    values = jax.random.normal(jax.random.fold_in(key, 3), (GROUPS, SEQ, D), jnp.float32)
    return jnp.clip(values, -60.0, 60.0).astype(jnp.bfloat16)


def block_scale(rng, extent, shards, smallest, high):
    level, own = 1.0, jax.random.fold_in(rng, 6)
    for position, parts in shards:
        draws = jnp.exp(jax.random.uniform(jax.random.fold_in(own, position), (parts,), jnp.float32, smallest / len(shards), high / len(shards)))
        level = level * jnp.repeat(draws, extent[position] // parts).reshape([-1 if axis == position else 1 for axis in range(len(extent))])
    return level


def bell_draw(rng, shape, scale, most, cuts=(), kind=jnp.bfloat16):
    values = jax.random.normal(rng, shape, jnp.float32) * scale
    if len(cuts) > 0:
        values = block_scale(rng, shape, cuts, -0.22, 0.18) * values
    return jnp.clip(values, min=-most, max=most).astype(kind)


def setup_inputs(seed: int = 0) -> dict:
    key_list = jax.random.split(jax.random.key(seed), 8)
    tokens = draw_tokens(jax.random.fold_in(key_list[7], 71), 0)
    doc_lengths = draw_doc_lengths(jax.random.fold_in(key_list[7], 71), 0)
    picked = draw_picked(jax.random.fold_in(key_list[7], 71), 0)
    w_query = bell_draw(key_list[3], (D, HEADS * HEAD_DIM), D ** -0.5, 0.125, ((1, 2),))
    w_key = bell_draw(key_list[4], (D, KV_HEADS * HEAD_DIM), D ** -0.5, 0.125)
    w_value = bell_draw(key_list[5], (D, KV_HEADS * HEAD_DIM), D ** -0.5, 0.125)
    w_out = bell_draw(key_list[6], (HEADS * HEAD_DIM, D), (HEADS * HEAD_DIM) ** -0.5, 0.1875)
    return dict(tokens=tokens, doc_lengths=doc_lengths, picked=picked, w_query=w_query, w_key=w_key, w_value=w_value, w_out=w_out)


def rotate(values_in, positions):
    half = values_in.shape[-1] // 2
    inverse = 10000.0 ** (-jnp.arange(half, dtype=jnp.float32) / half)
    angles = positions.astype(jnp.float32)[:, None] * inverse[None, :]
    cosine = jnp.cos(angles)[:, None, :]
    sine = jnp.sin(angles)[:, None, :]
    first = values_in[..., :half]
    second = values_in[..., half:]
    return jnp.concatenate([first * cosine - second * sine, second * cosine + first * sine], axis=-1)


def doc_of(positions, ends):
    return jnp.sum((positions[..., None] >= ends).astype(jnp.int32), axis=-1)


def one_group(tokens, doc_lengths, picked, w_query, w_key, w_value, w_out):
    seq = tokens.shape[0]
    positions = jnp.arange(seq, dtype=jnp.int32)
    ends = jnp.cumsum(doc_lengths).astype(jnp.int32)
    queries = rotate(jnp.dot(tokens, w_query, preferred_element_type=jnp.float32).reshape(seq, HEADS, HEAD_DIM), positions).astype(jnp.bfloat16)
    keys = rotate(jnp.dot(tokens, w_key, preferred_element_type=jnp.float32).reshape(seq, KV_HEADS, HEAD_DIM), positions).astype(jnp.bfloat16)
    values = jnp.dot(tokens, w_value, preferred_element_type=jnp.float32).astype(jnp.bfloat16).reshape(seq, KV_HEADS, HEAD_DIM)
    queries, keys, values = lax.optimization_barrier((queries, keys, values))
    group = HEADS // KV_HEADS
    offsets = jnp.arange(BLOCK, dtype=jnp.int32)

    def attend_block(index):
        start = (index * BLOCK).astype(jnp.int32)
        rows = lax.dynamic_slice_in_dim(queries, start, BLOCK, 0)
        query_pos = start + offsets
        slots = picked[index]
        key_pos = (jnp.maximum(slots, 0)[:, None] * BLOCK + offsets[None, :]).reshape(-1).astype(jnp.int32)
        block_keys = keys[key_pos].astype(jnp.float32)
        block_values = values[key_pos].astype(jnp.float32)
        filled = jnp.repeat(slots >= 0, BLOCK)
        live = filled[None, :] & (key_pos[None, :] <= query_pos[:, None]) & (doc_of(key_pos, ends)[None, :] == doc_of(query_pos, ends)[:, None])
        grouped = rows.astype(jnp.float32).reshape(BLOCK, KV_HEADS, group, HEAD_DIM)
        scores = jnp.einsum('qngd,knd->ngqk', grouped, block_keys) * (HEAD_DIM ** -0.5)
        scores = jnp.where(live[None, None], scores, -jnp.inf)
        highest = jnp.max(scores, axis=-1, keepdims=True)
        weights = jnp.exp(scores - highest)
        total = jnp.sum(weights, axis=-1)
        rounded = lax.optimization_barrier(weights.astype(jnp.bfloat16))
        summed = jnp.einsum('ngqk,knd->qngd', rounded.astype(jnp.float32), block_values)
        result = summed / jnp.transpose(total, (2, 0, 1))[..., None]
        return result.astype(jnp.bfloat16).reshape(BLOCK, HEADS * HEAD_DIM)

    attended = lax.map(attend_block, jnp.arange(seq // BLOCK, dtype=jnp.int32)).reshape(seq, HEADS * HEAD_DIM)
    return jnp.dot(attended, w_out, preferred_element_type=jnp.float32).astype(jnp.bfloat16)


def reference(tokens, doc_lengths, picked, w_query, w_key, w_value, w_out):
    def run(index):
        return one_group(tokens[index], doc_lengths[index], picked[index], w_query, w_key, w_value, w_out)

    return lax.map(run, jnp.arange(tokens.shape[0], dtype=jnp.int32))
```

```python
import functools
import math

import jax
import jax.numpy as jnp
import numpy as np
from jax import lax
from jax.experimental import pallas as pl
from jax.experimental.pallas import tpu as pltpu
from jax.sharding import PartitionSpec as P

HEAD_DIM = 64
BLOCK = 32
LANES = 128
SPAN = 64
HOT = 2
NEAR = 2
STEP = 2
CHUNK = 256
MESH = pl.DeviceIdType.MESH
SCALE = float(HEAD_DIM ** -0.5 * np.log2(np.e))
FAR_OFF = 1 << 30
F32 = jnp.float32
BF16 = jnp.bfloat16


def tables(rows, count):
    lane = np.arange(LANES)
    half = HEAD_DIM // 2
    inverse = (10000.0 ** (-(lane % half) / half)).astype(np.float32).astype(np.float64)
    sign = np.where(lane % HEAD_DIM < half, -1.0, 1.0)
    row = np.arange(rows)[:, None] * inverse
    start = (np.arange(count) * rows)[:, None] * inverse
    inner = np.stack([np.cos(row), np.sin(row) * sign]).astype(np.float32)
    outer = np.zeros((count, 8, LANES), np.float32)
    outer[:, 0] = np.cos(start)
    outer[:, 1] = np.sin(start) * sign
    return inner, outer


def iota(shape, axis):
    return lax.broadcasted_iota(jnp.int32, shape, axis)


def dot_t(a, b):
    return lax.dot_general(a, b, (((1,), (1,)), ((), ())), preferred_element_type=F32)


def dot(a, b):
    return jnp.dot(a, b, preferred_element_type=F32)


def swap(x):
    return pltpu.roll(x, HEAD_DIM, 1)


def kernel(
    n, near, far, tok_hbm, doc_hbm, pick_hbm, wq_hbm, wk_hbm, wv_hbm, wo_hbm, inner_hbm, outer_hbm, out,
    tok, doc, pick, wq, wkv, wo, inner, outer, names, names_in, kv_all, kv_own, near_in, near_keys, pack, hot_in,
    ids, ids_in, bias, vt, q_all, acc, top, att, att_in, partial,
    load_sem, name_s, name_r, near_s, near_r, hot_s, hot_r, ids_s, ids_r, att_s, att_r,
):
    kv = lax.axis_index("kv")
    tp = lax.axis_index("tp")
    rows = tok.shape[0]
    blocks = rows // BLOCK
    heads = wq.shape[1] // HEAD_DIM
    mine = wo.shape[1]
    pad = names.shape[1]
    kept = HOT * BLOCK
    lead = tp == 1

    before_near = jnp.minimum(kv, near)
    before_far = jnp.clip(kv - near, 0, far)
    after_near = jnp.minimum(n - 1 - kv, near)
    after_far = jnp.clip(n - 1 - kv - near, 0, far)
    names_out = jnp.where(lead, before_far, 0)
    hots_out = jnp.where(lead, after_far, 0)

    barrier = pltpu.get_barrier_semaphore()

    def greet_near(i, _):
        pl.semaphore_signal(barrier, inc=1, device_id={"kv": kv - 1 - i}, device_id_type=MESH)
        return 0

    def greet_far(i, _):
        pl.semaphore_signal(barrier, inc=1, device_id={"kv": kv + 1 + near + i}, device_id_type=MESH)
        return 0

    lax.fori_loop(0, before_near, greet_near, 0)
    lax.fori_loop(0, hots_out, greet_far, 0)
    pl.semaphore_signal(barrier, inc=1, device_id={"tp": 1 - tp}, device_id_type=MESH)

    pairs = [
        (pick_hbm, pick), (tok_hbm.at[0], tok), (wk_hbm, wkv.at[:, 0:LANES]), (wv_hbm, wkv.at[:, LANES:]),
        (inner_hbm, inner), (outer_hbm.at[kv], outer), (doc_hbm, doc), (wq_hbm, wq),
        (wo_hbm.at[pl.ds(tp * mine, mine)], wo.at[0]), (wo_hbm.at[pl.ds((1 - tp) * mine, mine)], wo.at[1]),
    ]
    loads = [pltpu.make_async_copy(a, b, load_sem.at[i]) for i, (a, b) in enumerate(pairs)]
    for load in loads:
        load.start()
    l_pick, l_tok, l_wk, l_wv, l_in, l_out, l_doc, l_wq, l_wo0, l_wo1 = loads

    def clear_near(i, _):
        near_in[i] = jnp.zeros(near_in.shape[1:], BF16)
        return 0

    def clear_far(i, _):
        hot_in[i] = jnp.zeros(hot_in.shape[1:], BF16)
        ids_in[i] = jnp.zeros(ids_in.shape[1:], F32)
        return 0

    lax.fori_loop(before_near, near, clear_near, 0)
    lax.fori_loop(before_far, far, clear_far, 0)

    l_pick.wait()
    reach = near + far
    slot_rows = [pick[b] for b in range(blocks)]
    index = iota((reach * pad, slot_rows[0].shape[1]), 0)
    owner = kv - 1 - index // pad
    wanted = jnp.where((owner >= 0) & (index % pad < blocks), owner * blocks + index % pad, -9)
    hit = slot_rows[0] == wanted
    for b in range(1, blocks):
        hit = hit | (slot_rows[b] == wanted)
    flags = jnp.max(jnp.where(hit, 1.0, 0.0), axis=1, keepdims=True)
    names[...] = jnp.broadcast_to(flags, (reach * pad, LANES)).reshape(names.shape)

    l_in.wait()
    l_out.wait()
    cos_o, sin_o = outer[0:1, :], outer[1:2, :]
    cos_i, sin_i = inner[0], inner[1]
    cosine = cos_o * cos_i - sin_o * sin_i
    sine = sin_o * cos_i + cos_o * sin_i
    lane = iota((rows, LANES), 1)
    low = lane < HEAD_DIM
    first = lane % HEAD_DIM < HEAD_DIM // 2
    quarter = HEAD_DIM // 2

    def rotate(x):
        other = jnp.where(first, pltpu.roll(x, LANES - quarter, 1), pltpu.roll(x, quarter, 1))
        return x * cosine + other * sine

    l_tok.wait()
    l_wk.wait()
    l_wv.wait()
    both = dot(tok[...], wkv[...])
    keys = rotate(both[:, 0:LANES])
    values = both[:, LANES:]
    kv_all[0] = jnp.where(low, keys, swap(values))
    kv_all[1] = jnp.where(low, swap(keys), values)
    kv_own[...] = kv_all[tp].astype(BF16)

    pl.semaphore_wait(barrier, after_near + names_out + 1)

    def name_copy(i):
        return pltpu.make_async_remote_copy(
            src_ref=names.at[near + i], dst_ref=names_in.at[i], send_sem=name_s.at[i], recv_sem=name_r.at[i],
            device_id={"kv": kv - 1 - near - i}, device_id_type=MESH)

    def near_copy(i):
        return pltpu.make_async_remote_copy(
            src_ref=kv_own, dst_ref=near_in.at[i], send_sem=near_s.at[i], recv_sem=near_r.at[i],
            device_id={"kv": kv + 1 + i}, device_id_type=MESH)

    def hot_copy(i, t):
        return pltpu.make_async_remote_copy(
            src_ref=pack.at[t], dst_ref=hot_in.at[i], send_sem=hot_s.at[i, t], recv_sem=hot_r.at[i],
            device_id={"kv": kv + 1 + near + i, "tp": t}, device_id_type=MESH)

    def ids_copy(i, t):
        return pltpu.make_async_remote_copy(
            src_ref=ids, dst_ref=ids_in.at[i], send_sem=ids_s.at[i, t], recv_sem=ids_r.at[i],
            device_id={"kv": kv + 1 + near + i, "tp": t}, device_id_type=MESH)

    def name_send(i, _):
        name_copy(i).start()
        return 0

    def near_send(i, _):
        near_copy(i).start()
        return 0

    lax.fori_loop(0, names_out, name_send, 0)
    lax.fori_loop(0, after_near, near_send, 0)

    l_wq.wait()
    queries = dot(tok[...], wq[...])
    spans = rows // SPAN
    for p in range(heads // 2):
        turned = rotate(queries[:, p * LANES:(p + 1) * LANES])
        even = jnp.where(low, turned, 0.0).astype(BF16)
        odd = jnp.where(low, swap(turned), 0.0).astype(BF16)
        for r in range(spans):
            base = (p * spans + r) * LANES
            q_all[base:base + SPAN, :] = even[r * SPAN:(r + 1) * SPAN]
            q_all[base + SPAN:base + LANES, :] = odd[r * SPAN:(r + 1) * SPAN]

    l_doc.wait()
    tile_lane = iota((1, LANES), 1) % SPAN
    upper = iota((8, LANES), 1) % SPAN >= BLOCK
    q_pos = [kv * rows + r * SPAN + tile_lane for r in range(spans)]
    q_start = [jnp.zeros((1, LANES), jnp.int32) for _ in range(spans)]
    end = jnp.int32(0)
    for i in range(doc.shape[1]):
        end = end + doc[0, i]
        q_start = [jnp.where(pos >= end, end, s) for pos, s in zip(q_pos, q_start)]
    place = iota((BLOCK, LANES), 0)

    def set_bias(key_block, count, causal):
        found = []
        for b in range(blocks):
            same = slot_rows[b] == key_block[:, 0:slot_rows[b].shape[1]]
            found.append(jnp.max(jnp.where(same, 1.0, 0.0), axis=1, keepdims=True))
        for r in range(spans):
            named = jnp.where(upper, found[2 * r + 1], found[2 * r])
            floor = jnp.where(named > 0.5, q_start[r] - key_block * BLOCK, FAR_OFF)
            for k in range(count):
                live = place >= floor[k:k + 1, :]
                if causal:
                    live = live & (place <= q_pos[r] - (kv * rows + k * BLOCK))
                bias[k * BLOCK:(k + 1) * BLOCK, r * LANES:(r + 1) * LANES] = jnp.where(live, 0.0, -jnp.inf)

    def set_values(block):
        count = block.shape[0]
        vt[0:HEAD_DIM, 0:count] = jnp.transpose(block.astype(F32))[HEAD_DIM:, :].astype(BF16)

    def score(c, block):
        return dot_t(block, q_all[c * CHUNK:(c + 1) * CHUNK, :])

    def absorb(c, scores, fresh):
        count = scores.shape[0]
        cut = slice(c * CHUNK, (c + 1) * CHUNK)
        tiles = []
        for t in range(CHUNK // LANES):
            r = (c * (CHUNK // LANES) + t) % spans
            tiles.append(scores[:, t * LANES:(t + 1) * LANES] + bias[0:count, r * LANES:(r + 1) * LANES])
        scores = jnp.concatenate(tiles, axis=1)
        highest = jnp.max(scores, axis=0, keepdims=True)
        if not fresh:
            old = top[:, cut]
            highest = jnp.maximum(highest, old)
        weights = jnp.exp2((scores - highest) * SCALE).astype(BF16)
        summed = dot(vt[:, 0:count], weights)
        if not fresh:
            summed = summed + acc[:, cut] * jnp.exp2((old - highest) * SCALE)
        acc[:, cut] = summed
        top[:, cut] = highest

    def attend(begin, stop, block, fresh, after=None):
        ready = score(begin, block)
        for c in range(begin, stop):
            now = ready
            if c + 1 < stop:
                ready = score(c + 1, block)
            absorb(c, now, fresh)
            if after is not None:
                after(c)

    chunks = heads * rows // CHUNK
    vt[HEAD_DIM:, :] = jnp.ones((vt.shape[0] - HEAD_DIM, vt.shape[1]), BF16)
    local_block = iota((8, LANES), 0)
    set_bias(jnp.where(local_block < blocks, kv * blocks + local_block, -2), blocks, True)
    set_values(kv_all[tp])
    own = kv_own[...]
    attend(0, chunks, own, True)

    def choose(flag, base):
        rank = jnp.zeros((1, LANES), F32)
        weight = [[], []]
        label = [jnp.zeros((1, LANES), F32) for _ in range(HOT)]
        for b in range(blocks):
            for s in range(HOT):
                one = jnp.where((flag[b] > 0.5) & (rank == s), 1.0, 0.0)
                weight[s].append(one)
                label[s] = label[s] + one * (b + 1)
            rank = rank + flag[b]
        return weight, label

    def gather(weight, block):
        total = block(0) * weight[0]
        for b in range(1, blocks):
            total = total + block(b) * weight[b]
        return total

    @pl.when(lead)
    def _():
        def name_take(i, total):
            name_copy(i).wait_recv()
            return total + names_in[i]

        total = lax.fori_loop(0, after_far, name_take, jnp.zeros(names.shape[1:], F32))
        total = jnp.where(total > 0.5, 1.0, 0.0)
        weight, label = choose([total[b:b + 1, :] for b in range(blocks)], 0)
        for s in range(HOT):
            ids[s:s + 1, :] = label[s]
            for t in range(2):
                part = gather(weight[s], lambda b: kv_all[t, b * BLOCK:(b + 1) * BLOCK, :])
                pack[t, s * BLOCK:(s + 1) * BLOCK, :] = part.astype(BF16)

        def hot_send(i, _):
            for t in range(2):
                ids_copy(i, t).start()
            for t in range(2):
                hot_copy(i, t).start()
            return 0

        lax.fori_loop(0, after_far, hot_send, 0)

    def near_wait(i, _):
        near_copy(i).wait_recv()
        return 0

    def key_blocks(labels):
        found = [jnp.where(v > 0.5, base + v.astype(jnp.int32) - 1, -2) for base, v in labels]
        found += [jnp.full((1, LANES), -2, jnp.int32)] * (8 - len(found))
        return jnp.concatenate(found, axis=0)

    chosen = [choose([names[i, b:b + 1, :] for b in range(blocks)], 0) for i in range(near)]
    set_bias(key_blocks([((kv - 1 - i) * blocks, v) for i in range(near) for v in chosen[i][1]]), near * HOT, False)
    lax.fori_loop(0, before_near, near_wait, 0)
    for i in range(near):
        for s in range(HOT):
            part = gather(chosen[i][0][s], lambda b: near_in[i, b * BLOCK:(b + 1) * BLOCK, :].astype(F32))
            at = (i * HOT + s) * BLOCK
            near_keys[at:at + BLOCK, :] = part.astype(BF16)
    block = near_keys[...]
    set_values(block)
    attend(0, chunks, block, False)

    def att_copy(h):
        return pltpu.make_async_remote_copy(
            src_ref=att.at[h], dst_ref=att_in.at[h], send_sem=att_s.at[h], recv_sem=att_r.at[h],
            device_id={"tp": 1 - tp}, device_id_type=MESH)

    def ids_wait(i, _):
        ids_copy(i, tp).wait_recv()
        return 0

    def hot_wait(i, _):
        hot_copy(i, tp).wait_recv()
        return 0

    lax.fori_loop(0, before_far, ids_wait, 0)
    width = att.shape[2]
    halves = att.shape[0]

    def far_bias(start):
        labels = [((kv - 1 - near - start - i) * blocks, ids_in[start + i, s:s + 1, :]) for i in range(STEP) for s in range(HOT)]
        set_bias(key_blocks(labels), STEP * HOT, False)

    def far_block(start):
        block = hot_in[pl.ds(start, STEP)].reshape(STEP * kept, LANES)
        set_values(block)
        return block

    steps = far // STEP
    if steps > 1:
        lax.fori_loop(0, before_far, hot_wait, 0)

        def far_step(g, _):
            far_bias(g * STEP)
            block = far_block(g * STEP)
            attend(0, chunks, block, False)
            return 0

        lax.fori_loop(0, steps - 1, far_step, 0)
    far_bias((steps - 1) * STEP)
    if steps == 1:
        lax.fori_loop(0, before_far, hot_wait, 0)
    block = far_block((steps - 1) * STEP)
    low_tile = iota((SPAN, LANES), 1) < HEAD_DIM

    def finish(c):
        if (c + 1) * halves % chunks:
            return
        h = (c + 1) * halves // chunks - 1
        for p in range(h * heads // 2 // halves, (h + 1) * heads // 2 // halves):
            for r in range(spans):
                t = p * spans + r
                cut = slice(t * LANES, (t + 1) * LANES)
                part = acc[0:HEAD_DIM, cut] * (1.0 / acc[HEAD_DIM:HEAD_DIM + 1, cut])
                turned = jnp.transpose(jnp.concatenate([part, part], axis=0))
                part = jnp.where(low_tile, turned[0:SPAN], turned[SPAN:])
                at = p * LANES - h * width
                att[h, r * SPAN:(r + 1) * SPAN, at:at + LANES] = part.astype(BF16)
        att_copy(h).start()

    attend(0, chunks, block, False, finish)

    l_wo0.wait()
    columns = wo.shape[2]
    piece = columns // 4
    for c in range(4):
        cut = slice(c * piece, (c + 1) * piece)
        value = dot(att[0], wo[0, 0:width, cut])
        for h in range(1, halves):
            value += dot(att[h], wo[0, h * width:(h + 1) * width, cut])
        partial[:, cut] = value
    l_wo1.wait()
    for h in range(halves):
        att_copy(h).wait_recv()
    for c in range(4):
        cut = slice(c * piece, (c + 1) * piece)
        value = partial[:, cut]
        for h in range(halves):
            value += dot(att_in[h], wo[1, h * width:(h + 1) * width, cut])
        out[0, :, cut] = value.astype(BF16)

    def name_done(i, _):
        name_copy(i).wait_send()
        return 0

    def near_done(i, _):
        near_copy(i).wait_send()
        return 0

    def hot_done(i, _):
        for t in range(2):
            ids_copy(i, t).wait_send()
            hot_copy(i, t).wait_send()
        return 0

    lax.fori_loop(0, names_out, name_done, 0)
    lax.fori_loop(0, after_near, near_done, 0)
    lax.fori_loop(0, hots_out, hot_done, 0)
    for h in range(halves):
        att_copy(h).wait_send()


def solution(mesh):
    n = mesh.shape["kv"]

    def shards(tokens, doc_lengths, picked, w_query, w_key, w_value, w_out):
        _, rows, d = tokens.shape
        blocks = rows // BLOCK
        pad = -(-blocks // 8) * 8
        q_cols = w_query.shape[1]
        heads = q_cols // HEAD_DIM
        columns = w_out.shape[1]
        inner, outer = tables(rows, n)
        width = q_cols // 2
        dma = pltpu.SemaphoreType.DMA
        payload = HOT * BLOCK
        reach = min(n, (n * rows // 2 + rows - 2) // rows)
        near = NEAR
        far = -(-max(reach - near, 1) // STEP) * STEP
        most = max(rows, near * payload, STEP * payload)
        operands = (tokens, doc_lengths, jnp.transpose(picked, (1, 0, 2)), w_query, w_key, w_value, w_out, inner, outer)
        operands = [pltpu.with_memory_space_constraint(jnp.asarray(x), pltpu.HBM) for x in operands]
        return pl.pallas_call(
            functools.partial(kernel, n, near, far),
            out_shape=jax.ShapeDtypeStruct((1, rows, columns), BF16),
            in_specs=[pl.BlockSpec(memory_space=pltpu.HBM)] * 9,
            out_specs=pl.BlockSpec(memory_space=pltpu.VMEM),
            scratch_shapes=[
                pltpu.VMEM((rows, d), BF16),
                pltpu.SMEM(doc_lengths.shape, jnp.int32),
                pltpu.VMEM((blocks, 1, picked.shape[2]), jnp.int32),
                pltpu.VMEM(w_query.shape, BF16),
                pltpu.VMEM((d, 2 * LANES), BF16),
                pltpu.VMEM((2, w_out.shape[0] // 2, columns), BF16),
                pltpu.VMEM(inner.shape, F32),
                pltpu.VMEM(outer.shape[1:], F32),
                pltpu.VMEM((near + far, pad, LANES), F32),
                pltpu.VMEM((far, pad, LANES), F32),
                pltpu.VMEM((2, rows, LANES), F32),
                pltpu.VMEM((rows, LANES), BF16),
                pltpu.VMEM((near, rows, LANES), BF16),
                pltpu.VMEM((near * payload, LANES), BF16),
                pltpu.VMEM((2, payload, LANES), BF16),
                pltpu.VMEM((far, payload, LANES), BF16),
                pltpu.VMEM((HOT, LANES), F32),
                pltpu.VMEM((far, HOT, LANES), F32),
                pltpu.VMEM((most, rows // SPAN * LANES), F32),
                pltpu.VMEM((HEAD_DIM + 16, most), BF16),
                pltpu.VMEM((heads * rows, LANES), BF16),
                pltpu.VMEM((HEAD_DIM + 16, heads * rows), F32),
                pltpu.VMEM((1, heads * rows), F32),
                pltpu.VMEM((2, rows, width), BF16),
                pltpu.VMEM((2, rows, width), BF16),
                pltpu.VMEM((rows, columns), F32),
                dma((10,)), dma((far,)), dma((far,)), dma((near,)), dma((near,)),
                dma((far, 2)), dma((far,)), dma((far, 2)), dma((far,)), dma((2,)), dma((2,)),
            ],
            compiler_params=pltpu.CompilerParams(
                collective_id=0, has_side_effects=True, vmem_limit_bytes=28 * 1024 * 1024
            ),
        )(*operands)

    placed = (P("dp", "kv", None), P("dp", None), P("dp", "kv", None), P(None, "tp"), P(), P(), P())
    return jax.shard_map(
        shards, mesh=mesh, in_specs=placed, out_specs=P("dp", "kv", None), check_vma=False
    )
```

```python
import functools
import math

import jax
import jax.numpy as jnp
import numpy as np
from jax import lax
from jax.experimental import pallas as pl
from jax.experimental.pallas import tpu as pltpu
from jax.sharding import PartitionSpec as P

HEAD_DIM = 64
BLOCK = 32
LANES = 128
SPAN = 64
HOT = 2
NEAR = 2
STEP = 2
CHUNK = 256
MESH = pl.DeviceIdType.MESH
SCALE = float(HEAD_DIM ** -0.5 * np.log2(np.e))
FAR_OFF = 1 << 30
F32 = jnp.float32
BF16 = jnp.bfloat16


def tables(rows, count):
    lane = np.arange(LANES)
    half = HEAD_DIM // 2
    inverse = (10000.0 ** (-(lane % half) / half)).astype(np.float32).astype(np.float64)
    sign = np.where(lane % HEAD_DIM < half, -1.0, 1.0)
    row = np.arange(rows)[:, None] * inverse
    start = (np.arange(count) * rows)[:, None] * inverse
    inner = np.stack([np.cos(row), np.sin(row) * sign]).astype(np.float32)
    outer = np.zeros((count, 8, LANES), np.float32)
    outer[:, 0] = np.cos(start)
    outer[:, 1] = np.sin(start) * sign
    return inner, outer


def iota(shape, axis):
    return lax.broadcasted_iota(jnp.int32, shape, axis)


def dot_t(a, b):
    return lax.dot_general(a, b, (((1,), (1,)), ((), ())), preferred_element_type=F32)


def dot(a, b):
    return jnp.dot(a, b, preferred_element_type=F32)


def swap(x):
    return pltpu.roll(x, HEAD_DIM, 1)


def kernel(
    n, near, far, tok_hbm, doc_hbm, pick_hbm, wq_hbm, wk_hbm, wv_hbm, wo_hbm, inner_hbm, outer_hbm, out,
    tok, doc, pick, wq, wkv, wo, inner, outer, names, names_in, kv_all, kv_own, near_in, near_keys, pack, hot_in,
    ids, ids_in, bias, vt, q_all, acc, top, att, att_in, partial,
    load_sem, name_s, name_r, near_s, near_r, hot_s, hot_r, ids_s, ids_r, att_s, att_r,
):
    kv = lax.axis_index("kv")
    tp = lax.axis_index("tp")
    rows = tok.shape[0]
    blocks = rows // BLOCK
    heads = wq.shape[1] // HEAD_DIM
    mine = wo.shape[1]
    pad = names.shape[1]
    kept = HOT * BLOCK
    lead = tp == 1

    before_near = jnp.minimum(kv, near)
    before_far = jnp.clip(kv - near, 0, far)
    after_near = jnp.minimum(n - 1 - kv, near)
    after_far = jnp.clip(n - 1 - kv - near, 0, far)
    names_out = jnp.where(lead, before_far, 0)
    hots_out = jnp.where(lead, after_far, 0)

    barrier = pltpu.get_barrier_semaphore()

    def greet_near(i, _):
        pl.semaphore_signal(barrier, inc=1, device_id={"kv": kv - 1 - i}, device_id_type=MESH)
        return 0

    def greet_far(i, _):
        pl.semaphore_signal(barrier, inc=1, device_id={"kv": kv + 1 + near + i}, device_id_type=MESH)
        return 0

    lax.fori_loop(0, before_near, greet_near, 0)
    lax.fori_loop(0, hots_out, greet_far, 0)
    pl.semaphore_signal(barrier, inc=1, device_id={"tp": 1 - tp}, device_id_type=MESH)

    pairs = [
        (pick_hbm, pick), (tok_hbm.at[0], tok), (wk_hbm, wkv.at[:, 0:LANES]), (wv_hbm, wkv.at[:, LANES:]),
        (inner_hbm, inner), (outer_hbm.at[kv], outer), (doc_hbm, doc), (wq_hbm, wq),
        (wo_hbm.at[pl.ds(tp * mine, mine)], wo.at[0]), (wo_hbm.at[pl.ds((1 - tp) * mine, mine)], wo.at[1]),
    ]
    loads = [pltpu.make_async_copy(a, b, load_sem.at[i]) for i, (a, b) in enumerate(pairs)]
    for load in loads:
        load.start()
    l_pick, l_tok, l_wk, l_wv, l_in, l_out, l_doc, l_wq, l_wo0, l_wo1 = loads

    def clear_near(i, _):
        near_in[i] = jnp.zeros(near_in.shape[1:], BF16)
        return 0

    def clear_far(i, _):
        hot_in[i] = jnp.zeros(hot_in.shape[1:], BF16)
        ids_in[i] = jnp.zeros(ids_in.shape[1:], F32)
        return 0

    lax.fori_loop(before_near, near, clear_near, 0)
    lax.fori_loop(before_far, far, clear_far, 0)

    l_pick.wait()
    reach = near + far
    slot_rows = [pick[b] for b in range(blocks)]
    index = iota((reach * pad, slot_rows[0].shape[1]), 0)
    owner = kv - 1 - index // pad
    wanted = jnp.where((owner >= 0) & (index % pad < blocks), owner * blocks + index % pad, -9)
    hit = slot_rows[0] == wanted
    for b in range(1, blocks):
        hit = hit | (slot_rows[b] == wanted)
    flags = jnp.max(jnp.where(hit, 1.0, 0.0), axis=1, keepdims=True)
    names[...] = jnp.broadcast_to(flags, (reach * pad, LANES)).reshape(names.shape)

    pl.semaphore_wait(barrier, after_near + names_out + 1)

    def name_copy(i):
        return pltpu.make_async_remote_copy(
            src_ref=names.at[near + i], dst_ref=names_in.at[i], send_sem=name_s.at[i], recv_sem=name_r.at[i],
            device_id={"kv": kv - 1 - near - i}, device_id_type=MESH)

    def near_copy(i):
        return pltpu.make_async_remote_copy(
            src_ref=kv_own, dst_ref=near_in.at[i], send_sem=near_s.at[i], recv_sem=near_r.at[i],
            device_id={"kv": kv + 1 + i}, device_id_type=MESH)

    def hot_copy(i, t):
        return pltpu.make_async_remote_copy(
            src_ref=pack.at[t], dst_ref=hot_in.at[i], send_sem=hot_s.at[i, t], recv_sem=hot_r.at[i],
            device_id={"kv": kv + 1 + near + i, "tp": t}, device_id_type=MESH)

    def ids_copy(i, t):
        return pltpu.make_async_remote_copy(
            src_ref=ids, dst_ref=ids_in.at[i], send_sem=ids_s.at[i, t], recv_sem=ids_r.at[i],
            device_id={"kv": kv + 1 + near + i, "tp": t}, device_id_type=MESH)

    def name_send(i, _):
        name_copy(i).start()
        return 0

    def near_send(i, _):
        near_copy(i).start()
        return 0

    lax.fori_loop(0, names_out, name_send, 0)

    l_in.wait()
    l_out.wait()
    cos_o, sin_o = outer[0:1, :], outer[1:2, :]
    cos_i, sin_i = inner[0], inner[1]
    cosine = cos_o * cos_i - sin_o * sin_i
    sine = sin_o * cos_i + cos_o * sin_i
    lane = iota((rows, LANES), 1)
    low = lane < HEAD_DIM
    first = lane % HEAD_DIM < HEAD_DIM // 2
    quarter = HEAD_DIM // 2

    def rotate(x):
        other = jnp.where(first, pltpu.roll(x, LANES - quarter, 1), pltpu.roll(x, quarter, 1))
        return x * cosine + other * sine

    l_tok.wait()
    l_wk.wait()
    l_wv.wait()
    both = dot(tok[...], wkv[...])
    keys = rotate(both[:, 0:LANES])
    values = both[:, LANES:]
    kv_all[0] = jnp.where(low, keys, swap(values))
    kv_all[1] = jnp.where(low, swap(keys), values)
    kv_own[...] = kv_all[tp].astype(BF16)

    lax.fori_loop(0, after_near, near_send, 0)
    l_wq.wait()
    queries = dot(tok[...], wq[...])
    main = rows // LANES
    tail = rows % LANES
    kinds = [m for m in range(main) for _ in range(2)] + [main] * (tail > 0)
    per = len(kinds)
    for p in range(heads // 2):
        turned = rotate(queries[:, p * LANES:(p + 1) * LANES])
        flat = jnp.transpose(turned[0:main * LANES])
        for m in range(main):
            for e in range(2):
                at = (p * per + 2 * m + e) * LANES
                part = flat[e * HEAD_DIM:(e + 1) * HEAD_DIM, m * LANES:(m + 1) * LANES]
                q_all[:, at:at + LANES] = part.astype(BF16)
        if tail:
            rest = turned[main * LANES:]
            both = jnp.transpose(jnp.concatenate([rest, swap(rest)], axis=0))
            at = (p * per + per - 1) * LANES
            q_all[:, at:at + LANES] = both[0:HEAD_DIM].astype(BF16)

    l_doc.wait()
    lane_row = iota((1, LANES), 1)
    wide_row = iota((8, LANES), 1)
    q_row = [m * LANES + lane_row for m in range(main)] + [main * LANES + lane_row % SPAN] * (tail > 0)
    wide_q = [m * LANES + wide_row for m in range(main)] + [main * LANES + wide_row % SPAN] * (tail > 0)
    q_pos = [kv * rows + row for row in q_row]
    q_start = [jnp.zeros((1, LANES), jnp.int32) for _ in q_row]
    end = jnp.int32(0)
    for i in range(doc.shape[1]):
        end = end + doc[0, i]
        q_start = [jnp.where(pos >= end, end, s) for pos, s in zip(q_pos, q_start)]
    place = iota((BLOCK, LANES), 0)

    def set_bias(key_block, count, causal):
        found = []
        for b in range(blocks):
            same = slot_rows[b] == key_block[:, 0:slot_rows[b].shape[1]]
            found.append(jnp.max(jnp.where(same, 1.0, 0.0), axis=1, keepdims=True))
        for r in range(len(q_row)):
            begin = r * LANES // BLOCK
            stop = min(begin + LANES // BLOCK, blocks)
            named = found[begin]
            for b in range(begin + 1, stop):
                named = jnp.where(wide_q[r] >= b * BLOCK, found[b], named)
            floor = jnp.where(named > 0.5, q_start[r] - key_block * BLOCK, FAR_OFF)
            for k in range(count):
                live = place >= floor[k:k + 1, :]
                if causal:
                    live = live & (place <= q_pos[r] - (kv * rows + k * BLOCK))
                bias[k * BLOCK:(k + 1) * BLOCK, r * LANES:(r + 1) * LANES] = jnp.where(live, 0.0, -jnp.inf)

    def set_values(block):
        count = block.shape[0]
        vt[0:HEAD_DIM, 0:count] = jnp.transpose(block.astype(F32))[HEAD_DIM:, :].astype(BF16)

    def score(c, block):
        return dot(block[:, 0:HEAD_DIM], q_all[:, c * CHUNK:(c + 1) * CHUNK])

    def absorb(c, scores, fresh):
        count = scores.shape[0]
        cut = slice(c * CHUNK, (c + 1) * CHUNK)
        tiles = []
        for t in range(CHUNK // LANES):
            r = kinds[(c * (CHUNK // LANES) + t) % per]
            tiles.append(scores[:, t * LANES:(t + 1) * LANES] + bias[0:count, r * LANES:(r + 1) * LANES])
        scores = jnp.concatenate(tiles, axis=1)
        highest = jnp.max(scores, axis=0, keepdims=True)
        if not fresh:
            old = top[:, cut]
            highest = jnp.maximum(highest, old)
        weights = jnp.exp2((scores - highest) * SCALE).astype(BF16)
        summed = dot(vt[:, 0:count], weights)
        if not fresh:
            summed = summed + acc[:, cut] * jnp.exp2((old - highest) * SCALE)
        acc[:, cut] = summed
        top[:, cut] = highest

    def attend(begin, stop, block, fresh, after=None):
        ready = score(begin, block)
        for c in range(begin, stop):
            now = ready
            if c + 1 < stop:
                ready = score(c + 1, block)
            absorb(c, now, fresh)
            if after is not None:
                after(c)

    chunks = heads * rows // CHUNK
    vt[HEAD_DIM:, :] = jnp.ones((vt.shape[0] - HEAD_DIM, vt.shape[1]), BF16)
    local_block = iota((8, LANES), 0)
    set_bias(jnp.where(local_block < blocks, kv * blocks + local_block, -2), blocks, True)
    set_values(kv_all[tp])
    own = kv_own[...]
    attend(0, chunks, own, True)

    def choose(flag, base):
        rank = jnp.zeros((1, LANES), F32)
        weight = [[], []]
        label = [jnp.zeros((1, LANES), F32) for _ in range(HOT)]
        for b in range(blocks):
            for s in range(HOT):
                one = jnp.where((flag[b] > 0.5) & (rank == s), 1.0, 0.0)
                weight[s].append(one)
                label[s] = label[s] + one * (b + 1)
            rank = rank + flag[b]
        return weight, label

    def gather(weight, block):
        total = block(0) * weight[0]
        for b in range(1, blocks):
            total = total + block(b) * weight[b]
        return total

    @pl.when(lead)
    def _():
        def name_take(i, total):
            name_copy(i).wait_recv()
            return total + names_in[i]

        total = lax.fori_loop(0, after_far, name_take, jnp.zeros(names.shape[1:], F32))
        total = jnp.where(total > 0.5, 1.0, 0.0)
        weight, label = choose([total[b:b + 1, :] for b in range(blocks)], 0)
        for s in range(HOT):
            ids[s:s + 1, :] = label[s]
            for t in range(2):
                part = gather(weight[s], lambda b: kv_all[t, b * BLOCK:(b + 1) * BLOCK, :])
                pack[t, s * BLOCK:(s + 1) * BLOCK, :] = part.astype(BF16)

        def hot_send(i, _):
            for t in range(2):
                ids_copy(i, t).start()
            for t in range(2):
                hot_copy(i, t).start()
            return 0

        lax.fori_loop(0, after_far, hot_send, 0)

    def near_wait(i, _):
        near_copy(i).wait_recv()
        return 0

    def key_blocks(labels):
        found = [jnp.where(v > 0.5, base + v.astype(jnp.int32) - 1, -2) for base, v in labels]
        found += [jnp.full((1, LANES), -2, jnp.int32)] * (8 - len(found))
        return jnp.concatenate(found, axis=0)

    chosen = [choose([names[i, b:b + 1, :] for b in range(blocks)], 0) for i in range(near)]
    set_bias(key_blocks([((kv - 1 - i) * blocks, v) for i in range(near) for v in chosen[i][1]]), near * HOT, False)
    lax.fori_loop(0, before_near, near_wait, 0)
    for i in range(near):
        for s in range(HOT):
            part = gather(chosen[i][0][s], lambda b: near_in[i, b * BLOCK:(b + 1) * BLOCK, :].astype(F32))
            at = (i * HOT + s) * BLOCK
            near_keys[at:at + BLOCK, :] = part.astype(BF16)
    block = near_keys[...]
    set_values(block)
    attend(0, chunks, block, False)

    def att_copy(h):
        return pltpu.make_async_remote_copy(
            src_ref=att.at[h], dst_ref=att_in.at[h], send_sem=att_s.at[h], recv_sem=att_r.at[h],
            device_id={"tp": 1 - tp}, device_id_type=MESH)

    def ids_wait(i, _):
        ids_copy(i, tp).wait_recv()
        return 0

    def hot_wait(i, _):
        hot_copy(i, tp).wait_recv()
        return 0

    lax.fori_loop(0, before_far, ids_wait, 0)
    width = att.shape[2]
    halves = att.shape[0]

    def far_bias(start):
        labels = [((kv - 1 - near - start - i) * blocks, ids_in[start + i, s:s + 1, :]) for i in range(STEP) for s in range(HOT)]
        set_bias(key_blocks(labels), STEP * HOT, False)

    def far_block(start):
        block = hot_in[pl.ds(start, STEP)].reshape(STEP * kept, LANES)
        set_values(block)
        return block

    steps = far // STEP
    if steps > 1:
        lax.fori_loop(0, before_far, hot_wait, 0)

        def far_step(g, _):
            far_bias(g * STEP)
            block = far_block(g * STEP)
            attend(0, chunks, block, False)
            return 0

        lax.fori_loop(0, steps - 1, far_step, 0)
    far_bias((steps - 1) * STEP)
    if steps == 1:
        lax.fori_loop(0, before_far, hot_wait, 0)
    block = far_block((steps - 1) * STEP)
    low_tile = iota((SPAN, LANES), 1) < HEAD_DIM

    def finish(c):
        if (c + 1) * halves % chunks:
            return
        h = (c + 1) * halves // chunks - 1
        for p in range(h * heads // 2 // halves, (h + 1) * heads // 2 // halves):
            at = p * LANES - h * width

            def scaled(t):
                cut = slice((p * per + t) * LANES, (p * per + t + 1) * LANES)
                return acc[0:HEAD_DIM, cut] * (1.0 / acc[HEAD_DIM:HEAD_DIM + 1, cut])

            for m in range(main):
                part = jnp.transpose(jnp.concatenate([scaled(2 * m), scaled(2 * m + 1)], axis=0))
                att[h, m * LANES:(m + 1) * LANES, at:at + LANES] = part.astype(BF16)
            if tail:
                part = scaled(per - 1)
                turned = jnp.transpose(jnp.concatenate([part, part], axis=0))
                part = jnp.where(low_tile, turned[0:SPAN], turned[SPAN:])
                att[h, main * LANES:, at:at + LANES] = part.astype(BF16)
        att_copy(h).start()

    attend(0, chunks, block, False, finish)

    l_wo0.wait()
    columns = wo.shape[2]
    piece = columns // 4
    for c in range(4):
        cut = slice(c * piece, (c + 1) * piece)
        value = dot(att[0], wo[0, 0:width, cut])
        for h in range(1, halves):
            value += dot(att[h], wo[0, h * width:(h + 1) * width, cut])
        partial[:, cut] = value
    l_wo1.wait()
    att_copy(0).wait_recv()
    for h in range(halves - 1):
        if h:
            att_copy(h).wait_recv()
        for c in range(4):
            cut = slice(c * piece, (c + 1) * piece)
            partial[:, cut] += dot(att_in[h], wo[1, h * width:(h + 1) * width, cut])
    att_copy(halves - 1).wait_recv()
    for c in range(4):
        cut = slice(c * piece, (c + 1) * piece)
        value = partial[:, cut] + dot(att_in[halves - 1], wo[1, (halves - 1) * width:halves * width, cut])
        out[0, :, cut] = value.astype(BF16)

    def name_done(i, _):
        name_copy(i).wait_send()
        return 0

    def near_done(i, _):
        near_copy(i).wait_send()
        return 0

    def hot_done(i, _):
        for t in range(2):
            ids_copy(i, t).wait_send()
            hot_copy(i, t).wait_send()
        return 0

    lax.fori_loop(0, names_out, name_done, 0)
    lax.fori_loop(0, after_near, near_done, 0)
    lax.fori_loop(0, hots_out, hot_done, 0)
    for h in range(halves):
        att_copy(h).wait_send()


def solution(mesh):
    n = mesh.shape["kv"]

    def shards(tokens, doc_lengths, picked, w_query, w_key, w_value, w_out):
        _, rows, d = tokens.shape
        blocks = rows // BLOCK
        pad = -(-blocks // 8) * 8
        q_cols = w_query.shape[1]
        heads = q_cols // HEAD_DIM
        columns = w_out.shape[1]
        inner, outer = tables(rows, n)
        width = q_cols // 2
        dma = pltpu.SemaphoreType.DMA
        payload = HOT * BLOCK
        reach = min(n, (n * rows // 2 + rows - 2) // rows)
        near = NEAR
        far = -(-max(reach - near, 1) // STEP) * STEP
        most = max(rows, near * payload, STEP * payload)
        operands = (tokens, doc_lengths, jnp.transpose(picked, (1, 0, 2)), w_query, w_key, w_value, w_out, inner, outer)
        operands = [pltpu.with_memory_space_constraint(jnp.asarray(x), pltpu.HBM) for x in operands]
        return pl.pallas_call(
            functools.partial(kernel, n, near, far),
            out_shape=jax.ShapeDtypeStruct((1, rows, columns), BF16),
            in_specs=[pl.BlockSpec(memory_space=pltpu.HBM)] * 9,
            out_specs=pl.BlockSpec(memory_space=pltpu.VMEM),
            scratch_shapes=[
                pltpu.VMEM((rows, d), BF16),
                pltpu.SMEM(doc_lengths.shape, jnp.int32),
                pltpu.VMEM((blocks, 1, picked.shape[2]), jnp.int32),
                pltpu.VMEM(w_query.shape, BF16),
                pltpu.VMEM((d, 2 * LANES), BF16),
                pltpu.VMEM((2, w_out.shape[0] // 2, columns), BF16),
                pltpu.VMEM(inner.shape, F32),
                pltpu.VMEM(outer.shape[1:], F32),
                pltpu.VMEM((near + far, pad, LANES), F32),
                pltpu.VMEM((far, pad, LANES), F32),
                pltpu.VMEM((2, rows, LANES), F32),
                pltpu.VMEM((rows, LANES), BF16),
                pltpu.VMEM((near, rows, LANES), BF16),
                pltpu.VMEM((near * payload, LANES), BF16),
                pltpu.VMEM((2, payload, LANES), BF16),
                pltpu.VMEM((far, payload, LANES), BF16),
                pltpu.VMEM((HOT, LANES), F32),
                pltpu.VMEM((far, HOT, LANES), F32),
                pltpu.VMEM((most, -(-rows // LANES) * LANES), F32),
                pltpu.VMEM((HEAD_DIM + 16, most), BF16),
                pltpu.VMEM((HEAD_DIM, heads * rows), BF16),
                pltpu.VMEM((HEAD_DIM + 16, heads * rows), F32),
                pltpu.VMEM((1, heads * rows), F32),
                pltpu.VMEM((2, rows, width), BF16),
                pltpu.VMEM((2, rows, width), BF16),
                pltpu.VMEM((rows, columns), F32),
                dma((10,)), dma((far,)), dma((far,)), dma((near,)), dma((near,)),
                dma((far, 2)), dma((far,)), dma((far, 2)), dma((far,)), dma((2,)), dma((2,)),
            ],
            compiler_params=pltpu.CompilerParams(
                collective_id=0, has_side_effects=True, vmem_limit_bytes=28 * 1024 * 1024
            ),
        )(*operands)

    placed = (P("dp", "kv", None), P("dp", None), P("dp", "kv", None), P(None, "tp"), P(), P(), P())
    return jax.shard_map(
        shards, mesh=mesh, in_specs=placed, out_specs=P("dp", "kv", None), check_vma=False
    )
```

```python
import functools
import math

import jax
import jax.numpy as jnp
import numpy as np
from jax import lax
from jax.experimental import pallas as pl
from jax.experimental.pallas import tpu as pltpu
from jax.sharding import PartitionSpec as P

HEAD_DIM = 64
BLOCK = 32
LANES = 128
SPAN = 64
HOT = 2
NEAR = 2
STEP = 2
CHUNK = 256
DEPTH = 6
MESH = pl.DeviceIdType.MESH
SCALE = float(HEAD_DIM ** -0.5 * np.log2(np.e))
FAR_OFF = 1 << 30
F32 = jnp.float32
BF16 = jnp.bfloat16


def tables(rows, count):
    lane = np.arange(LANES)
    half = HEAD_DIM // 2
    inverse = (10000.0 ** (-(lane % half) / half)).astype(np.float32).astype(np.float64)
    sign = np.where(lane % HEAD_DIM < half, -1.0, 1.0)
    row = np.arange(rows)[:, None] * inverse
    start = (np.arange(count) * rows)[:, None] * inverse
    inner = np.stack([np.cos(row), np.sin(row) * sign]).astype(np.float32)
    outer = np.zeros((count, 8, LANES), np.float32)
    outer[:, 0] = np.cos(start)
    outer[:, 1] = np.sin(start) * sign
    return inner, outer


def iota(shape, axis):
    return lax.broadcasted_iota(jnp.int32, shape, axis)


def dot_t(a, b):
    return lax.dot_general(a, b, (((1,), (1,)), ((), ())), preferred_element_type=F32)


def dot(a, b):
    return jnp.dot(a, b, preferred_element_type=F32)


def swap(x):
    return pltpu.roll(x, HEAD_DIM, 1)


def kernel(
    n, near, far, tok_hbm, doc_hbm, pick_hbm, wq_hbm, wk_hbm, wv_hbm, wo_hbm, inner_hbm, outer_hbm, out,
    tok, doc, pick, wq, wkv, wo, inner, outer, names, names_in, kv_all, kv_own, near_in, near_keys, pack, hot_in,
    bias, vt, q_all, acc, top, att, att_in, partial,
    load_sem, name_s, name_r, near_s, near_r, hot_s, hot_r, att_s, att_r,
):
    kv = lax.axis_index("kv")
    tp = lax.axis_index("tp")
    rows = tok.shape[0]
    blocks = rows // BLOCK
    heads = wq.shape[1] // HEAD_DIM
    mine = wo.shape[1]
    pad = names.shape[1]
    kept = HOT * BLOCK
    lead = tp == 1

    before_near = jnp.minimum(kv, near)
    before_far = jnp.clip(kv - near, 0, far)
    after_near = jnp.minimum(n - 1 - kv, near)
    after_far = jnp.clip(n - 1 - kv - near, 0, far)
    names_out = jnp.where(lead, before_far, 0)
    hots_out = jnp.where(lead, after_far, 0)

    barrier = pltpu.get_barrier_semaphore()

    def greet_near(i, _):
        pl.semaphore_signal(barrier, inc=1, device_id={"kv": kv - 1 - i}, device_id_type=MESH)
        return 0

    def greet_far(i, _):
        pl.semaphore_signal(barrier, inc=1, device_id={"kv": kv + 1 + near + i}, device_id_type=MESH)
        return 0

    lax.fori_loop(0, before_near, greet_near, 0)
    lax.fori_loop(0, hots_out, greet_far, 0)
    pl.semaphore_signal(barrier, inc=1, device_id={"tp": 1 - tp}, device_id_type=MESH)

    pairs = [
        (pick_hbm, pick), (tok_hbm.at[0], tok), (wk_hbm, wkv.at[:, 0:LANES]), (wv_hbm, wkv.at[:, LANES:]),
        (inner_hbm, inner), (outer_hbm.at[kv], outer), (doc_hbm, doc), (wq_hbm, wq),
        (wo_hbm.at[pl.ds(tp * mine, mine)], wo.at[0]), (wo_hbm.at[pl.ds((1 - tp) * mine, mine)], wo.at[1]),
    ]
    loads = [pltpu.make_async_copy(a, b, load_sem.at[i]) for i, (a, b) in enumerate(pairs)]
    for load in loads:
        load.start()
    l_pick, l_tok, l_wk, l_wv, l_in, l_out, l_doc, l_wq, l_wo0, l_wo1 = loads

    def clear_near(i, _):
        near_in[i] = jnp.zeros(near_in.shape[1:], BF16)
        return 0

    def clear_far(i, _):
        hot_in[i] = jnp.zeros(hot_in.shape[1:], BF16)
        return 0

    lax.fori_loop(before_near, near, clear_near, 0)
    lax.fori_loop(before_far, far, clear_far, 0)

    l_pick.wait()
    reach = near + far
    slot_rows = [pick[b] for b in range(blocks)]
    index = iota((reach * pad, slot_rows[0].shape[1]), 0)
    owner = kv - 1 - index // pad
    wanted = jnp.where((owner >= 0) & (index % pad < blocks), owner * blocks + index % pad, -9)
    hit = slot_rows[0] == wanted
    for b in range(1, blocks):
        hit = hit | (slot_rows[b] == wanted)
    flags = jnp.max(jnp.where(hit, 1.0, 0.0), axis=1, keepdims=True)
    names[...] = jnp.broadcast_to(flags, (reach * pad, LANES)).reshape(names.shape)

    pl.semaphore_wait(barrier, after_near + names_out + 1)

    def name_copy(i):
        return pltpu.make_async_remote_copy(
            src_ref=names.at[near + i], dst_ref=names_in.at[i], send_sem=name_s.at[i], recv_sem=name_r.at[i],
            device_id={"kv": kv - 1 - near - i}, device_id_type=MESH)

    def near_copy(i):
        return pltpu.make_async_remote_copy(
            src_ref=kv_own, dst_ref=near_in.at[i], send_sem=near_s.at[i], recv_sem=near_r.at[i],
            device_id={"kv": kv + 1 + i}, device_id_type=MESH)

    def hot_copy(i, t):
        return pltpu.make_async_remote_copy(
            src_ref=pack.at[i, t], dst_ref=hot_in.at[i], send_sem=hot_s.at[i, t], recv_sem=hot_r.at[i],
            device_id={"kv": kv + 1 + near + i, "tp": t}, device_id_type=MESH)

    def name_send(i, _):
        name_copy(i).start()
        return 0

    def near_send(i, _):
        near_copy(i).start()
        return 0

    lax.fori_loop(0, names_out, name_send, 0)

    l_in.wait()
    l_out.wait()
    cos_o, sin_o = outer[0:1, :], outer[1:2, :]
    cos_i, sin_i = inner[0], inner[1]
    cosine = cos_o * cos_i - sin_o * sin_i
    sine = sin_o * cos_i + cos_o * sin_i
    lane = iota((rows, LANES), 1)
    low = lane < HEAD_DIM
    first = lane % HEAD_DIM < HEAD_DIM // 2
    quarter = HEAD_DIM // 2

    def rotate(x):
        other = jnp.where(first, pltpu.roll(x, LANES - quarter, 1), pltpu.roll(x, quarter, 1))
        return x * cosine + other * sine

    l_tok.wait()
    l_wk.wait()
    l_wv.wait()
    both = dot(tok[...], wkv[...])
    keys = rotate(both[:, 0:LANES])
    values = both[:, LANES:]
    kv_all[0] = jnp.where(low, keys, swap(values))
    kv_all[1] = jnp.where(low, swap(keys), values)
    kv_own[...] = kv_all[tp].astype(BF16)

    lax.fori_loop(0, after_near, near_send, 0)
    l_wq.wait()
    queries = dot(tok[...], wq[...])
    main = rows // LANES
    tail = rows % LANES
    kinds = [m for m in range(main) for _ in range(2)] + [main] * (tail > 0)
    per = len(kinds)
    for p in range(heads // 2):
        turned = rotate(queries[:, p * LANES:(p + 1) * LANES])
        flat = jnp.transpose(turned[0:main * LANES])
        for m in range(main):
            for e in range(2):
                at = (p * per + 2 * m + e) * LANES
                part = flat[e * HEAD_DIM:(e + 1) * HEAD_DIM, m * LANES:(m + 1) * LANES]
                q_all[:, at:at + LANES] = part.astype(BF16)
        if tail:
            rest = turned[main * LANES:]
            both = jnp.transpose(jnp.concatenate([rest, swap(rest)], axis=0))
            at = (p * per + per - 1) * LANES
            q_all[:, at:at + LANES] = both[0:HEAD_DIM].astype(BF16)

    l_doc.wait()
    lane_row = iota((1, LANES), 1)
    wide_row = iota((8, LANES), 1)
    q_row = [m * LANES + lane_row for m in range(main)] + [main * LANES + lane_row % SPAN] * (tail > 0)
    wide_q = [m * LANES + wide_row for m in range(main)] + [main * LANES + wide_row % SPAN] * (tail > 0)
    q_pos = [kv * rows + row for row in q_row]
    q_start = [jnp.zeros((1, LANES), jnp.int32) for _ in q_row]
    end = jnp.int32(0)
    for i in range(doc.shape[1]):
        end = end + doc[0, i]
        q_start = [jnp.where(pos >= end, end, s) for pos, s in zip(q_pos, q_start)]
    place = iota((BLOCK, LANES), 0)

    def set_bias(key_block, count, causal):
        found = []
        for b in range(blocks):
            same = slot_rows[b] == key_block[:, 0:slot_rows[b].shape[1]]
            found.append(jnp.max(jnp.where(same, 1.0, 0.0), axis=1, keepdims=True))
        for r in range(len(q_row)):
            begin = r * LANES // BLOCK
            stop = min(begin + LANES // BLOCK, blocks)
            named = found[begin]
            for b in range(begin + 1, stop):
                named = jnp.where(wide_q[r] >= b * BLOCK, found[b], named)
            floor = jnp.where(named > 0.5, q_start[r] - key_block * BLOCK, FAR_OFF)
            for k in range(count):
                live = place >= floor[k:k + 1, :]
                if causal:
                    live = live & (place <= q_pos[r] - (kv * rows + k * BLOCK))
                bias[k * BLOCK:(k + 1) * BLOCK, r * LANES:(r + 1) * LANES] = jnp.where(live, 0.0, -jnp.inf)

    def set_values(block):
        count = block.shape[0]
        vt[0:HEAD_DIM, 0:count] = jnp.transpose(block)[HEAD_DIM:, :]

    def score(c, block):
        return dot(block[:, 0:HEAD_DIM], q_all[:, c * CHUNK:(c + 1) * CHUNK])

    def absorb(c, scores, fresh):
        count = scores.shape[0]
        cut = slice(c * CHUNK, (c + 1) * CHUNK)
        tiles = []
        for t in range(CHUNK // LANES):
            r = kinds[(c * (CHUNK // LANES) + t) % per]
            tiles.append(scores[:, t * LANES:(t + 1) * LANES] + bias[0:count, r * LANES:(r + 1) * LANES])
        scores = jnp.concatenate(tiles, axis=1)
        highest = jnp.max(scores, axis=0, keepdims=True)
        if not fresh:
            old = top[:, cut]
            highest = jnp.maximum(highest, old)
        weights = jnp.exp2((scores - highest) * SCALE).astype(BF16)
        summed = dot(vt[:, 0:count], weights)
        if not fresh:
            summed = summed + acc[:, cut] * jnp.exp2((old - highest) * SCALE)
        acc[:, cut] = summed
        top[:, cut] = highest

    def attend(begin, stop, block, fresh, after=None):
        ready = [score(c, block) for c in range(begin, min(begin + DEPTH, stop))]
        for c in range(begin, stop):
            now = ready.pop(0)
            if c + DEPTH < stop:
                ready.append(score(c + DEPTH, block))
            absorb(c, now, fresh)
            if after is not None:
                after(c)

    chunks = heads * rows // CHUNK
    vt[HEAD_DIM:, :] = jnp.ones((vt.shape[0] - HEAD_DIM, vt.shape[1]), BF16)
    local_block = iota((8, LANES), 0)
    set_bias(jnp.where(local_block < blocks, kv * blocks + local_block, -2), blocks, True)
    set_values(kv_own[...])
    def choose(flag):
        rank = jnp.zeros((1, LANES), F32)
        weight = [[], []]
        label = [jnp.zeros((1, LANES), F32) for _ in range(HOT)]
        for b in range(blocks):
            for s in range(HOT):
                one = jnp.where((flag[b] > 0.5) & (rank == s), 1.0, 0.0)
                weight[s].append(one)
                label[s] = label[s] + one * (b + 1)
            rank = rank + flag[b]
        return weight, label

    def gather(weight, block):
        total = block(0) * weight[0]
        for b in range(1, blocks):
            total = total + block(b) * weight[b]
        return total

    def choose_from(flags):
        return choose([flags[b:b + 1, :] for b in range(blocks)])

    def hot_send(i, _):
        name_copy(i).wait_recv()
        weight, _ = choose_from(names_in[i])
        for t in range(2):
            for s in range(HOT):
                part = gather(weight[s], lambda b: kv_all[t, b * BLOCK:(b + 1) * BLOCK, :])
                pack[i, t, s * BLOCK:(s + 1) * BLOCK, :] = part.astype(BF16)
            hot_copy(i, t).start()
        return 0

    ahead = kv % 2 == 1
    lax.fori_loop(0, jnp.where(ahead, 0, hots_out), hot_send, 0)

    own = kv_own[...]
    attend(0, chunks, own, True)
    lax.fori_loop(0, jnp.where(ahead, hots_out, 0), hot_send, 0)

    def near_wait(i, _):
        near_copy(i).wait_recv()
        return 0

    def key_blocks(labels):
        found = [jnp.where(v > 0.5, base + v.astype(jnp.int32) - 1, -2) for base, v in labels]
        found += [jnp.full((1, LANES), -2, jnp.int32)] * (8 - len(found))
        return jnp.concatenate(found, axis=0)

    chosen = [choose_from(names[i]) for i in range(near)]
    set_bias(key_blocks([((kv - 1 - i) * blocks, v) for i in range(near) for v in chosen[i][1]]), near * HOT, False)
    lax.fori_loop(0, before_near, near_wait, 0)
    for i in range(near):
        for s in range(HOT):
            part = gather(chosen[i][0][s], lambda b: near_in[i, b * BLOCK:(b + 1) * BLOCK, :].astype(F32))
            at = (i * HOT + s) * BLOCK
            near_keys[at:at + BLOCK, :] = part.astype(BF16)
    block = near_keys[...]
    set_values(block)
    attend(0, chunks, block, False)

    def att_copy(h):
        return pltpu.make_async_remote_copy(
            src_ref=att.at[h], dst_ref=att_in.at[h], send_sem=att_s.at[h], recv_sem=att_r.at[h],
            device_id={"tp": 1 - tp}, device_id_type=MESH)

    def hot_wait(i, _):
        hot_copy(i, tp).wait_recv()
        return 0

    width = att.shape[2]
    halves = att.shape[0]

    def far_bias(start):
        labels = []
        for i in range(STEP):
            _, label = choose_from(names[near + start + i])
            labels += [((kv - 1 - near - start - i) * blocks, v) for v in label]
        set_bias(key_blocks(labels), STEP * HOT, False)

    def far_block(start):
        block = hot_in[pl.ds(start, STEP)].reshape(STEP * kept, LANES)
        set_values(block)
        return block

    steps = far // STEP
    if steps > 1:
        lax.fori_loop(0, before_far, hot_wait, 0)

        def far_step(g, _):
            far_bias(g * STEP)
            block = far_block(g * STEP)
            attend(0, chunks, block, False)
            return 0

        lax.fori_loop(0, steps - 1, far_step, 0)
    far_bias((steps - 1) * STEP)
    if steps == 1:
        lax.fori_loop(0, before_far, hot_wait, 0)
    block = far_block((steps - 1) * STEP)
    low_tile = iota((SPAN, LANES), 1) < HEAD_DIM

    def finish(c):
        if (c + 1) * halves % chunks:
            return
        h = (c + 1) * halves // chunks - 1
        for p in range(h * heads // 2 // halves, (h + 1) * heads // 2 // halves):
            at = p * LANES - h * width

            def scaled(t):
                cut = slice((p * per + t) * LANES, (p * per + t + 1) * LANES)
                return (acc[0:HEAD_DIM, cut] * (1.0 / acc[HEAD_DIM:HEAD_DIM + 1, cut])).astype(BF16)

            for m in range(main):
                part = jnp.transpose(jnp.concatenate([scaled(2 * m), scaled(2 * m + 1)], axis=0))
                att[h, m * LANES:(m + 1) * LANES, at:at + LANES] = part
            if tail:
                part = scaled(per - 1)
                turned = jnp.transpose(jnp.concatenate([part, part], axis=0))
                part = jnp.where(low_tile, turned[0:SPAN], turned[SPAN:])
                att[h, main * LANES:, at:at + LANES] = part
        att_copy(h).start()

    attend(0, chunks, block, False, finish)

    l_wo0.wait()
    columns = wo.shape[2]
    piece = columns // 4
    for c in range(4):
        cut = slice(c * piece, (c + 1) * piece)
        value = dot(att[0], wo[0, 0:width, cut])
        for h in range(1, halves):
            value += dot(att[h], wo[0, h * width:(h + 1) * width, cut])
        partial[:, cut] = value
    l_wo1.wait()
    att_copy(0).wait_recv()
    for h in range(halves - 1):
        if h:
            att_copy(h).wait_recv()
        for c in range(4):
            cut = slice(c * piece, (c + 1) * piece)
            partial[:, cut] += dot(att_in[h], wo[1, h * width:(h + 1) * width, cut])
    att_copy(halves - 1).wait_recv()
    for c in range(4):
        cut = slice(c * piece, (c + 1) * piece)
        value = partial[:, cut] + dot(att_in[halves - 1], wo[1, (halves - 1) * width:halves * width, cut])
        out[0, :, cut] = value.astype(BF16)

    def name_done(i, _):
        name_copy(i).wait_send()
        return 0

    def near_done(i, _):
        near_copy(i).wait_send()
        return 0

    def hot_done(i, _):
        for t in range(2):
            hot_copy(i, t).wait_send()
        return 0

    lax.fori_loop(0, names_out, name_done, 0)
    lax.fori_loop(0, after_near, near_done, 0)
    lax.fori_loop(0, hots_out, hot_done, 0)
    for h in range(halves):
        att_copy(h).wait_send()


def solution(mesh):
    n = mesh.shape["kv"]

    def shards(tokens, doc_lengths, picked, w_query, w_key, w_value, w_out):
        _, rows, d = tokens.shape
        blocks = rows // BLOCK
        pad = -(-blocks // 8) * 8
        q_cols = w_query.shape[1]
        heads = q_cols // HEAD_DIM
        columns = w_out.shape[1]
        inner, outer = tables(rows, n)
        width = q_cols // 2
        dma = pltpu.SemaphoreType.DMA
        payload = HOT * BLOCK
        reach = min(n, (n * rows // 2 + rows - 2) // rows)
        near = NEAR
        far = -(-max(reach - near, 1) // STEP) * STEP
        most = max(rows, near * payload, STEP * payload)
        operands = (tokens, doc_lengths, jnp.transpose(picked, (1, 0, 2)), w_query, w_key, w_value, w_out, inner, outer)
        operands = [pltpu.with_memory_space_constraint(jnp.asarray(x), pltpu.HBM) for x in operands]
        return pl.pallas_call(
            functools.partial(kernel, n, near, far),
            out_shape=jax.ShapeDtypeStruct((1, rows, columns), BF16),
            in_specs=[pl.BlockSpec(memory_space=pltpu.HBM)] * 9,
            out_specs=pl.BlockSpec(memory_space=pltpu.VMEM),
            scratch_shapes=[
                pltpu.VMEM((rows, d), BF16),
                pltpu.SMEM(doc_lengths.shape, jnp.int32),
                pltpu.VMEM((blocks, 1, picked.shape[2]), jnp.int32),
                pltpu.VMEM(w_query.shape, BF16),
                pltpu.VMEM((d, 2 * LANES), BF16),
                pltpu.VMEM((2, w_out.shape[0] // 2, columns), BF16),
                pltpu.VMEM(inner.shape, F32),
                pltpu.VMEM(outer.shape[1:], F32),
                pltpu.VMEM((near + far, pad, LANES), F32),
                pltpu.VMEM((far, pad, LANES), F32),
                pltpu.VMEM((2, rows, LANES), F32),
                pltpu.VMEM((rows, LANES), BF16),
                pltpu.VMEM((near, rows, LANES), BF16),
                pltpu.VMEM((near * payload, LANES), BF16),
                pltpu.VMEM((far, 2, payload, LANES), BF16),
                pltpu.VMEM((far, payload, LANES), BF16),
                pltpu.VMEM((most, -(-rows // LANES) * LANES), F32),
                pltpu.VMEM((HEAD_DIM + 16, most), BF16),
                pltpu.VMEM((HEAD_DIM, heads * rows), BF16),
                pltpu.VMEM((HEAD_DIM + 16, heads * rows), F32),
                pltpu.VMEM((1, heads * rows), F32),
                pltpu.VMEM((2, rows, width), BF16),
                pltpu.VMEM((2, rows, width), BF16),
                pltpu.VMEM((rows, columns), F32),
                dma((10,)), dma((far,)), dma((far,)), dma((near,)), dma((near,)),
                dma((far, 2)), dma((far,)), dma((2,)), dma((2,)),
            ],
            compiler_params=pltpu.CompilerParams(
                collective_id=0, has_side_effects=True, vmem_limit_bytes=28 * 1024 * 1024
            ),
        )(*operands)

    placed = (P("dp", "kv", None), P("dp", None), P("dp", "kv", None), P(None, "tp"), P(), P(), P())
    return jax.shard_map(
        shards, mesh=mesh, in_specs=placed, out_specs=P("dp", "kv", None), check_vma=False
    )
```

```python
import functools
import math

import jax
import jax.numpy as jnp
import numpy as np
from jax import lax
from jax.experimental import pallas as pl
from jax.experimental.pallas import tpu as pltpu
from jax.sharding import PartitionSpec as P

HEAD_DIM = 64
BLOCK = 32
LANES = 128
SPAN = 64
HOT = 2
NEAR = 2
STEP = 2
CHUNK = 256
PIECES = 4
DEPTH = 6
MESH = pl.DeviceIdType.MESH
SCALE = float(HEAD_DIM ** -0.5 * np.log2(np.e))
FAR_OFF = 1 << 30
F32 = jnp.float32
BF16 = jnp.bfloat16


def tables(rows, count):
    lane = np.arange(LANES)
    half = HEAD_DIM // 2
    inverse = (10000.0 ** (-(lane % half) / half)).astype(np.float32).astype(np.float64)
    sign = np.where(lane % HEAD_DIM < half, -1.0, 1.0)
    row = np.arange(rows)[:, None] * inverse
    start = (np.arange(count) * rows)[:, None] * inverse
    inner = np.stack([np.cos(row), np.sin(row) * sign]).astype(np.float32)
    outer = np.zeros((count, 8, LANES), np.float32)
    outer[:, 0] = np.cos(start)
    outer[:, 1] = np.sin(start) * sign
    return inner, outer


def iota(shape, axis):
    return lax.broadcasted_iota(jnp.int32, shape, axis)


def dot_t(a, b):
    return lax.dot_general(a, b, (((1,), (1,)), ((), ())), preferred_element_type=F32)


def dot(a, b):
    return jnp.dot(a, b, preferred_element_type=F32)


def swap(x):
    return pltpu.roll(x, HEAD_DIM, 1)


def kernel(
    n, near, far, tok_hbm, doc_hbm, pick_hbm, wq_hbm, wk_hbm, wv_hbm, wo_hbm, inner_hbm, outer_hbm, partial, last, w_last,
    tok, doc, pick, wq, wkv, wo, inner, outer, names, names_in, kv_all, kv_own, near_in, near_keys, pack, hot_in,
    bias, vt, q_all, acc, top, att, att_in,
    load_sem, name_s, name_r, near_s, near_r, hot_s, hot_r, att_s, att_r,
):
    kv = lax.axis_index("kv")
    tp = lax.axis_index("tp")
    rows = tok.shape[0]
    blocks = rows // BLOCK
    heads = wq.shape[1] // HEAD_DIM
    width = att.shape[2]
    halves = att.shape[0]
    mine = halves * width
    pad = names.shape[1]
    kept = HOT * BLOCK
    lead = tp == 1

    before_near = jnp.minimum(kv, near)
    before_far = jnp.clip(kv - near, 0, far)
    after_near = jnp.minimum(n - 1 - kv, near)
    after_far = jnp.clip(n - 1 - kv - near, 0, far)
    names_out = jnp.where(lead, before_far, 0)
    hots_out = jnp.where(lead, after_far, 0)

    barrier = pltpu.get_barrier_semaphore()

    def greet_near(i, _):
        pl.semaphore_signal(barrier, inc=1, device_id={"kv": kv - 1 - i}, device_id_type=MESH)
        return 0

    def greet_far(i, _):
        pl.semaphore_signal(barrier, inc=1, device_id={"kv": kv + 1 + near + i}, device_id_type=MESH)
        return 0

    lax.fori_loop(0, before_near, greet_near, 0)
    lax.fori_loop(0, hots_out, greet_far, 0)
    pl.semaphore_signal(barrier, inc=1, device_id={"tp": 1 - tp}, device_id_type=MESH)

    pairs = [
        (pick_hbm, pick), (tok_hbm.at[0], tok), (wk_hbm, wkv.at[:, 0:LANES]), (wv_hbm, wkv.at[:, LANES:]),
        (inner_hbm, inner), (outer_hbm.at[kv], outer), (doc_hbm, doc), (wq_hbm, wq),
        (wo_hbm.at[pl.ds(tp * mine, mine)], wo.at[0:mine]),
        (wo_hbm.at[pl.ds((1 - tp) * mine, mine - width)], wo.at[mine:]),
        (wo_hbm.at[pl.ds((1 - tp) * mine + mine - width, width)], w_last),
    ]
    loads = [pltpu.make_async_copy(a, b, load_sem.at[i]) for i, (a, b) in enumerate(pairs)]
    for load in loads:
        load.start()
    l_pick, l_tok, l_wk, l_wv, l_in, l_out, l_doc, l_wq, l_wo0, l_wo1, l_wo2 = loads

    def clear_near(i, _):
        near_in[i] = jnp.zeros(near_in.shape[1:], BF16)
        return 0

    def clear_far(i, _):
        hot_in[i] = jnp.zeros(hot_in.shape[1:], BF16)
        return 0

    lax.fori_loop(before_near, near, clear_near, 0)
    lax.fori_loop(before_far, far, clear_far, 0)

    l_pick.wait()
    reach = near + far
    slot_rows = [pick[b] for b in range(blocks)]
    index = iota((reach * pad, slot_rows[0].shape[1]), 0)
    owner = kv - 1 - index // pad
    wanted = jnp.where((owner >= 0) & (index % pad < blocks), owner * blocks + index % pad, -9)
    hit = slot_rows[0] == wanted
    for b in range(1, blocks):
        hit = hit | (slot_rows[b] == wanted)
    flags = jnp.max(jnp.where(hit, 1.0, 0.0), axis=1, keepdims=True)
    names[...] = jnp.broadcast_to(flags, (reach * pad, LANES)).reshape(names.shape)

    pl.semaphore_wait(barrier, after_near + names_out + 1)

    def name_copy(i):
        return pltpu.make_async_remote_copy(
            src_ref=names.at[near + i], dst_ref=names_in.at[i], send_sem=name_s.at[i], recv_sem=name_r.at[i],
            device_id={"kv": kv - 1 - near - i}, device_id_type=MESH)

    def near_copy(i):
        return pltpu.make_async_remote_copy(
            src_ref=kv_own, dst_ref=near_in.at[i], send_sem=near_s.at[i], recv_sem=near_r.at[i],
            device_id={"kv": kv + 1 + i}, device_id_type=MESH)

    def hot_copy(i, t):
        return pltpu.make_async_remote_copy(
            src_ref=pack.at[i, t], dst_ref=hot_in.at[i], send_sem=hot_s.at[i, t], recv_sem=hot_r.at[i],
            device_id={"kv": kv + 1 + near + i, "tp": t}, device_id_type=MESH)

    def name_send(i, _):
        name_copy(i).start()
        return 0

    def near_send(i, _):
        near_copy(i).start()
        return 0

    lax.fori_loop(0, names_out, name_send, 0)

    l_in.wait()
    l_out.wait()
    cos_o, sin_o = outer[0:1, :], outer[1:2, :]
    cos_i, sin_i = inner[0], inner[1]
    cosine = cos_o * cos_i - sin_o * sin_i
    sine = sin_o * cos_i + cos_o * sin_i
    lane = iota((rows, LANES), 1)
    low = lane < HEAD_DIM
    first = lane % HEAD_DIM < HEAD_DIM // 2
    quarter = HEAD_DIM // 2

    def rotate(x):
        other = jnp.where(first, pltpu.roll(x, LANES - quarter, 1), pltpu.roll(x, quarter, 1))
        return x * cosine + other * sine

    l_tok.wait()
    l_wk.wait()
    l_wv.wait()
    both = dot(tok[...], wkv[...])
    keys = rotate(both[:, 0:LANES])
    values = both[:, LANES:]
    kv_all[0] = jnp.where(low, keys, swap(values))
    kv_all[1] = jnp.where(low, swap(keys), values)
    kv_own[...] = kv_all[tp].astype(BF16)

    lax.fori_loop(0, after_near, near_send, 0)
    l_wq.wait()
    queries = dot(tok[...], wq[...])
    main = rows // LANES
    tail = rows % LANES
    kinds = [m for m in range(main) for _ in range(2)] + [main] * (tail > 0)
    per = len(kinds)
    for p in range(heads // 2):
        turned = rotate(queries[:, p * LANES:(p + 1) * LANES])
        flat = jnp.transpose(turned[0:main * LANES])
        for m in range(main):
            for e in range(2):
                at = (p * per + 2 * m + e) * LANES
                part = flat[e * HEAD_DIM:(e + 1) * HEAD_DIM, m * LANES:(m + 1) * LANES]
                q_all[:, at:at + LANES] = part.astype(BF16)
        if tail:
            rest = turned[main * LANES:]
            both = jnp.transpose(jnp.concatenate([rest, swap(rest)], axis=0))
            at = (p * per + per - 1) * LANES
            q_all[:, at:at + LANES] = both[0:HEAD_DIM].astype(BF16)

    l_doc.wait()
    lane_row = iota((1, LANES), 1)
    wide_row = iota((8, LANES), 1)
    q_row = [m * LANES + lane_row for m in range(main)] + [main * LANES + lane_row % SPAN] * (tail > 0)
    wide_q = [m * LANES + wide_row for m in range(main)] + [main * LANES + wide_row % SPAN] * (tail > 0)
    q_pos = [kv * rows + row for row in q_row]
    q_start = [jnp.zeros((1, LANES), jnp.int32) for _ in q_row]
    end = jnp.int32(0)
    for i in range(doc.shape[1]):
        end = end + doc[0, i]
        q_start = [jnp.where(pos >= end, end, s) for pos, s in zip(q_pos, q_start)]
    place = iota((BLOCK, LANES), 0)

    def set_bias(key_block, count, causal):
        found = []
        for b in range(blocks):
            same = slot_rows[b] == key_block[:, 0:slot_rows[b].shape[1]]
            found.append(jnp.max(jnp.where(same, 1.0, 0.0), axis=1, keepdims=True))
        for r in range(len(q_row)):
            begin = r * LANES // BLOCK
            stop = min(begin + LANES // BLOCK, blocks)
            named = found[begin]
            for b in range(begin + 1, stop):
                named = jnp.where(wide_q[r] >= b * BLOCK, found[b], named)
            floor = jnp.where(named > 0.5, q_start[r] - key_block * BLOCK, FAR_OFF)
            for k in range(count):
                live = place >= floor[k:k + 1, :]
                if causal:
                    live = live & (place <= q_pos[r] - (kv * rows + k * BLOCK))
                bias[k * BLOCK:(k + 1) * BLOCK, r * LANES:(r + 1) * LANES] = jnp.where(live, 0.0, -jnp.inf)

    def set_values(block):
        count = block.shape[0]
        vt[0:HEAD_DIM, 0:count] = jnp.transpose(block)[HEAD_DIM:, :]

    def score(c, block):
        return dot(block[:, 0:HEAD_DIM], q_all[:, c * CHUNK:(c + 1) * CHUNK])

    def absorb(c, scores, fresh):
        count = scores.shape[0]
        cut = slice(c * CHUNK, (c + 1) * CHUNK)
        tiles = []
        for t in range(CHUNK // LANES):
            r = kinds[(c * (CHUNK // LANES) + t) % per]
            tiles.append(scores[:, t * LANES:(t + 1) * LANES] + bias[0:count, r * LANES:(r + 1) * LANES])
        scores = jnp.concatenate(tiles, axis=1)
        highest = jnp.max(scores, axis=0, keepdims=True)
        if not fresh:
            old = top[:, cut]
            highest = jnp.maximum(highest, old)
        weights = jnp.exp2((scores - highest) * SCALE).astype(BF16)
        summed = dot(vt[:, 0:count], weights)
        if not fresh:
            summed = summed + acc[:, cut] * jnp.exp2((old - highest) * SCALE)
        acc[:, cut] = summed
        top[:, cut] = highest

    def attend(begin, stop, block, fresh, after=None):
        ready = [score(c, block) for c in range(begin, min(begin + DEPTH, stop))]
        for c in range(begin, stop):
            now = ready.pop(0)
            if c + DEPTH < stop:
                ready.append(score(c + DEPTH, block))
            absorb(c, now, fresh)
            if after is not None:
                after(c)

    chunks = heads * rows // CHUNK
    vt[HEAD_DIM:, :] = jnp.ones((vt.shape[0] - HEAD_DIM, vt.shape[1]), BF16)
    local_block = iota((8, LANES), 0)
    set_bias(jnp.where(local_block < blocks, kv * blocks + local_block, -2), blocks, True)
    set_values(kv_own[...])
    def choose(flag):
        rank = jnp.zeros((1, LANES), F32)
        weight = [[], []]
        label = [jnp.zeros((1, LANES), F32) for _ in range(HOT)]
        for b in range(blocks):
            for s in range(HOT):
                one = jnp.where((flag[b] > 0.5) & (rank == s), 1.0, 0.0)
                weight[s].append(one)
                label[s] = label[s] + one * (b + 1)
            rank = rank + flag[b]
        return weight, label

    def gather(weight, block):
        total = block(0) * weight[0]
        for b in range(1, blocks):
            total = total + block(b) * weight[b]
        return total

    def choose_from(flags):
        return choose([flags[b:b + 1, :] for b in range(blocks)])

    def hot_send(i, _):
        name_copy(i).wait_recv()
        weight, _ = choose_from(names_in[i])
        for t in range(2):
            for s in range(HOT):
                part = gather(weight[s], lambda b: kv_all[t, b * BLOCK:(b + 1) * BLOCK, :])
                pack[i, t, s * BLOCK:(s + 1) * BLOCK, :] = part.astype(BF16)
            hot_copy(i, t).start()
        return 0

    ahead = kv % 2 == 1
    lax.fori_loop(0, jnp.where(ahead, 0, hots_out), hot_send, 0)

    own = kv_own[...]
    attend(0, chunks, own, True)
    lax.fori_loop(0, jnp.where(ahead, jnp.minimum(hots_out, 1), 0), hot_send, 0)

    def near_wait(i, _):
        near_copy(i).wait_recv()
        return 0

    def key_blocks(labels):
        found = [jnp.where(v > 0.5, base + v.astype(jnp.int32) - 1, -2) for base, v in labels]
        found += [jnp.full((1, LANES), -2, jnp.int32)] * (8 - len(found))
        return jnp.concatenate(found, axis=0)

    chosen = [choose_from(names[i]) for i in range(near)]
    set_bias(key_blocks([((kv - 1 - i) * blocks, v) for i in range(near) for v in chosen[i][1]]), near * HOT, False)
    lax.fori_loop(0, before_near, near_wait, 0)
    for i in range(near):
        for s in range(HOT):
            part = gather(chosen[i][0][s], lambda b: near_in[i, b * BLOCK:(b + 1) * BLOCK, :].astype(F32))
            at = (i * HOT + s) * BLOCK
            near_keys[at:at + BLOCK, :] = part.astype(BF16)
    block = near_keys[...]
    set_values(block)
    attend(0, chunks, block, False)

    lax.fori_loop(1, jnp.where(ahead, hots_out, 1), hot_send, 0)

    def att_copy(h):
        return pltpu.make_async_remote_copy(
            src_ref=att.at[h], dst_ref=att_in.at[h], send_sem=att_s.at[h], recv_sem=att_r.at[h],
            device_id={"tp": 1 - tp}, device_id_type=MESH)

    def hot_wait(i, _):
        hot_copy(i, tp).wait_recv()
        return 0


    def far_bias(start):
        labels = []
        for i in range(STEP):
            _, label = choose_from(names[near + start + i])
            labels += [((kv - 1 - near - start - i) * blocks, v) for v in label]
        set_bias(key_blocks(labels), STEP * HOT, False)

    def far_block(start):
        block = hot_in[pl.ds(start, STEP)].reshape(STEP * kept, LANES)
        set_values(block)
        return block

    steps = far // STEP
    if steps > 1:
        lax.fori_loop(0, before_far, hot_wait, 0)

        def far_step(g, _):
            far_bias(g * STEP)
            block = far_block(g * STEP)
            attend(0, chunks, block, False)
            return 0

        lax.fori_loop(0, steps - 1, far_step, 0)
    far_bias((steps - 1) * STEP)
    if steps == 1:
        lax.fori_loop(0, before_far, hot_wait, 0)
    block = far_block((steps - 1) * STEP)
    low_tile = iota((SPAN, LANES), 1) < HEAD_DIM

    def finish(c):
        if (c + 1) * halves % chunks:
            return
        h = (c + 1) * halves // chunks - 1
        for p in range(h * heads // 2 // halves, (h + 1) * heads // 2 // halves):
            at = p * LANES - h * width

            def scaled(t):
                cut = slice((p * per + t) * LANES, (p * per + t + 1) * LANES)
                return (acc[0:HEAD_DIM, cut] * (1.0 / acc[HEAD_DIM:HEAD_DIM + 1, cut])).astype(BF16)

            for m in range(main):
                part = jnp.transpose(jnp.concatenate([scaled(2 * m), scaled(2 * m + 1)], axis=0))
                att[h, m * LANES:(m + 1) * LANES, at:at + LANES] = part
            if tail:
                part = scaled(per - 1)
                turned = jnp.transpose(jnp.concatenate([part, part], axis=0))
                part = jnp.where(low_tile, turned[0:SPAN], turned[SPAN:])
                att[h, main * LANES:, at:at + LANES] = part
        att_copy(h).start()

    attend(0, chunks, block, False, finish)

    l_wo0.wait()
    columns = wo.shape[1]
    piece = columns // 4
    for c in range(4):
        cut = slice(c * piece, (c + 1) * piece)
        value = dot(att[0], wo[0:width, cut])
        for h in range(1, halves):
            value += dot(att[h], wo[h * width:(h + 1) * width, cut])
        partial[:, cut] = value
    l_wo1.wait()
    att_copy(0).wait_recv()
    for h in range(halves - 1):
        if h:
            att_copy(h).wait_recv()
        for c in range(4):
            cut = slice(c * piece, (c + 1) * piece)
            partial[:, cut] += dot(att_in[h], wo[mine + h * width:mine + (h + 1) * width, cut])
    att_copy(halves - 1).wait_recv()
    last[...] = att_in[halves - 1]
    l_wo2.wait()

    def name_done(i, _):
        name_copy(i).wait_send()
        return 0

    def near_done(i, _):
        near_copy(i).wait_send()
        return 0

    def hot_done(i, _):
        for t in range(2):
            hot_copy(i, t).wait_send()
        return 0

    lax.fori_loop(0, names_out, name_done, 0)
    lax.fori_loop(0, after_near, near_done, 0)
    lax.fori_loop(0, hots_out, hot_done, 0)
    for h in range(halves):
        att_copy(h).wait_send()


def finish(partial, last, weight, out, stage, sem):
    wide = stage.shape[2]
    stores = []
    for c in range(stage.shape[0]):
        cut = slice(c * wide, (c + 1) * wide)
        stage[c] = (partial[:, cut] + dot(last[...], weight[:, cut])).astype(BF16)
        store = pltpu.make_async_copy(stage.at[c], out.at[0, :, cut], sem.at[c])
        store.start()
        stores.append(store)
    for store in stores:
        store.wait()


def solution(mesh):
    n = mesh.shape["kv"]

    def shards(tokens, doc_lengths, picked, w_query, w_key, w_value, w_out):
        _, rows, d = tokens.shape
        blocks = rows // BLOCK
        pad = -(-blocks // 8) * 8
        q_cols = w_query.shape[1]
        heads = q_cols // HEAD_DIM
        columns = w_out.shape[1]
        inner, outer = tables(rows, n)
        width = q_cols // 2
        dma = pltpu.SemaphoreType.DMA
        payload = HOT * BLOCK
        reach = min(n, (n * rows // 2 + rows - 2) // rows)
        near = NEAR
        far = -(-max(reach - near, 1) // STEP) * STEP
        most = max(rows, near * payload, STEP * payload)
        operands = (tokens, doc_lengths, jnp.transpose(picked, (1, 0, 2)), w_query, w_key, w_value, w_out, inner, outer)
        operands = [pltpu.with_memory_space_constraint(jnp.asarray(x), pltpu.HBM) for x in operands]
        vmem = pl.BlockSpec(memory_space=pltpu.VMEM)
        parts = pl.pallas_call(
            functools.partial(kernel, n, near, far),
            out_shape=[
                jax.ShapeDtypeStruct((rows, columns), F32),
                jax.ShapeDtypeStruct((rows, width), BF16),
                jax.ShapeDtypeStruct((width, columns), BF16),
            ],
            in_specs=[pl.BlockSpec(memory_space=pltpu.HBM)] * 9,
            out_specs=[vmem] * 3,
            scratch_shapes=[
                pltpu.VMEM((rows, d), BF16),
                pltpu.SMEM(doc_lengths.shape, jnp.int32),
                pltpu.VMEM((blocks, 1, picked.shape[2]), jnp.int32),
                pltpu.VMEM(w_query.shape, BF16),
                pltpu.VMEM((d, 2 * LANES), BF16),
                pltpu.VMEM((w_out.shape[0] - width, columns), BF16),
                pltpu.VMEM(inner.shape, F32),
                pltpu.VMEM(outer.shape[1:], F32),
                pltpu.VMEM((near + far, pad, LANES), F32),
                pltpu.VMEM((far, pad, LANES), F32),
                pltpu.VMEM((2, rows, LANES), F32),
                pltpu.VMEM((rows, LANES), BF16),
                pltpu.VMEM((near, rows, LANES), BF16),
                pltpu.VMEM((near * payload, LANES), BF16),
                pltpu.VMEM((far, 2, payload, LANES), BF16),
                pltpu.VMEM((far, payload, LANES), BF16),
                pltpu.VMEM((most, -(-rows // LANES) * LANES), F32),
                pltpu.VMEM((HEAD_DIM + 16, most), BF16),
                pltpu.VMEM((HEAD_DIM, heads * rows), BF16),
                pltpu.VMEM((HEAD_DIM + 16, heads * rows), F32),
                pltpu.VMEM((1, heads * rows), F32),
                pltpu.VMEM((2, rows, width), BF16),
                pltpu.VMEM((2, rows, width), BF16),
                dma((11,)), dma((far,)), dma((far,)), dma((near,)), dma((near,)),
                dma((far, 2)), dma((far,)), dma((2,)), dma((2,)),
            ],
            compiler_params=pltpu.CompilerParams(
                collective_id=0, has_side_effects=True, vmem_limit_bytes=28 * 1024 * 1024
            ),
        )(*operands)
        return pl.pallas_call(
            finish,
            out_shape=jax.ShapeDtypeStruct((1, rows, columns), BF16),
            in_specs=[vmem] * 3,
            out_specs=pl.BlockSpec(memory_space=pltpu.HBM),
            scratch_shapes=[pltpu.VMEM((PIECES, rows, columns // PIECES), BF16), dma((PIECES,))],
            compiler_params=pltpu.CompilerParams(vmem_limit_bytes=8 * 1024 * 1024),
        )(*parts)

    placed = (P("dp", "kv", None), P("dp", None), P("dp", "kv", None), P(None, "tp"), P(), P(), P())
    return jax.shard_map(
        shards, mesh=mesh, in_specs=placed, out_specs=P("dp", "kv", None), check_vma=False
    )
```

```python
import functools
import math

import jax
import jax.numpy as jnp
import numpy as np
from jax import lax
from jax.experimental import pallas as pl
from jax.experimental.pallas import tpu as pltpu
from jax.sharding import PartitionSpec as P

HEAD_DIM = 64
BLOCK = 32
LANES = 128
SPAN = 64
HOT = 2
NEAR = 2
STEP = 2
CHUNK = 256
PIECES = 4
DEPTH = 6
MESH = pl.DeviceIdType.MESH
SCALE = float(HEAD_DIM ** -0.5 * np.log2(np.e))
FAR_OFF = 1 << 30
F32 = jnp.float32
BF16 = jnp.bfloat16


def tables(rows, count):
    lane = np.arange(LANES)
    half = HEAD_DIM // 2
    inverse = (10000.0 ** (-(lane % half) / half)).astype(np.float32).astype(np.float64)
    sign = np.where(lane % HEAD_DIM < half, -1.0, 1.0)
    row = np.arange(rows)[:, None] * inverse
    start = (np.arange(count) * rows)[:, None] * inverse
    inner = np.stack([np.cos(row), np.sin(row) * sign]).astype(np.float32)
    outer = np.zeros((count, 8, LANES), np.float32)
    outer[:, 0] = np.cos(start)
    outer[:, 1] = np.sin(start) * sign
    return inner, outer


def iota(shape, axis):
    return lax.broadcasted_iota(jnp.int32, shape, axis)


def dot_t(a, b):
    return lax.dot_general(a, b, (((1,), (1,)), ((), ())), preferred_element_type=F32)


def dot(a, b):
    return jnp.dot(a, b, preferred_element_type=F32)


def swap(x):
    return pltpu.roll(x, HEAD_DIM, 1)


def kernel(
    n, near, far, tok_hbm, doc_hbm, pick_hbm, wq_hbm, wk_hbm, wv_hbm, wo_hbm, inner_hbm, outer_hbm, partial, last, w_last,
    tok, doc, pick, wq, wkv, wo, inner, outer, names, names_in, kv_all, kv_own, near_in, near_keys, pack, hot_in,
    bias, vt, q_all, acc, top, att, att_in,
    load_sem, name_s, name_r, near_s, near_r, hot_s, hot_r, att_s, att_r,
):
    kv = lax.axis_index("kv")
    tp = lax.axis_index("tp")
    rows = tok.shape[0]
    blocks = rows // BLOCK
    heads = wq.shape[1] // HEAD_DIM
    width = att.shape[2]
    halves = att.shape[0]
    mine = halves * width
    pad = names.shape[1]
    kept = HOT * BLOCK
    lead = tp == 1

    before_near = jnp.minimum(kv, near)
    before_far = jnp.clip(kv - near, 0, far)
    after_near = jnp.minimum(n - 1 - kv, near)
    after_far = jnp.clip(n - 1 - kv - near, 0, far)
    names_out = jnp.where(lead, before_far, 0)
    hots_out = jnp.where(lead, after_far, 0)

    barrier = pltpu.get_barrier_semaphore()

    def greet_near(i, _):
        pl.semaphore_signal(barrier, inc=1, device_id={"kv": kv - 1 - i}, device_id_type=MESH)
        return 0

    def greet_far(i, _):
        pl.semaphore_signal(barrier, inc=1, device_id={"kv": kv + 1 + near + i}, device_id_type=MESH)
        return 0

    lax.fori_loop(0, before_near, greet_near, 0)
    lax.fori_loop(0, hots_out, greet_far, 0)
    pl.semaphore_signal(barrier, inc=1, device_id={"tp": 1 - tp}, device_id_type=MESH)

    pairs = [
        (pick_hbm, pick), (tok_hbm.at[0], tok), (wk_hbm, wkv.at[:, 0:LANES]), (wv_hbm, wkv.at[:, LANES:]),
        (inner_hbm, inner), (outer_hbm.at[kv], outer), (doc_hbm, doc), (wq_hbm, wq),
        (wo_hbm.at[pl.ds(tp * mine, mine)], wo.at[0:mine]),
        (wo_hbm.at[pl.ds((1 - tp) * mine, mine - width)], wo.at[mine:]),
        (wo_hbm.at[pl.ds((1 - tp) * mine + mine - width, width)], w_last),
    ]
    loads = [pltpu.make_async_copy(a, b, load_sem.at[i]) for i, (a, b) in enumerate(pairs)]
    for load in loads:
        load.start()
    l_pick, l_tok, l_wk, l_wv, l_in, l_out, l_doc, l_wq, l_wo0, l_wo1, l_wo2 = loads

    def clear_near(i, _):
        near_in[i] = jnp.zeros(near_in.shape[1:], BF16)
        return 0

    def clear_far(i, _):
        hot_in[i] = jnp.zeros(hot_in.shape[1:], BF16)
        return 0

    lax.fori_loop(before_near, near, clear_near, 0)
    lax.fori_loop(before_far, far, clear_far, 0)

    l_pick.wait()
    reach = near + far
    slot_rows = [pick[b] for b in range(blocks)]
    index = iota((reach * pad, slot_rows[0].shape[1]), 0)
    owner = kv - 1 - index // pad
    wanted = jnp.where((owner >= 0) & (index % pad < blocks), owner * blocks + index % pad, -9)
    hit = slot_rows[0] == wanted
    for b in range(1, blocks):
        hit = hit | (slot_rows[b] == wanted)
    flags = jnp.max(jnp.where(hit, 1.0, 0.0), axis=1, keepdims=True)
    names[...] = jnp.broadcast_to(flags, (reach * pad, LANES)).reshape(names.shape)

    pl.semaphore_wait(barrier, after_near + names_out + 1)

    def name_copy(i):
        return pltpu.make_async_remote_copy(
            src_ref=names.at[near + i], dst_ref=names_in.at[i], send_sem=name_s.at[i], recv_sem=name_r.at[i],
            device_id={"kv": kv - 1 - near - i}, device_id_type=MESH)

    def near_copy(i):
        return pltpu.make_async_remote_copy(
            src_ref=kv_own, dst_ref=near_in.at[i], send_sem=near_s.at[i], recv_sem=near_r.at[i],
            device_id={"kv": kv + 1 + i}, device_id_type=MESH)

    def hot_copy(i, t):
        return pltpu.make_async_remote_copy(
            src_ref=pack.at[i, t], dst_ref=hot_in.at[i], send_sem=hot_s.at[i, t], recv_sem=hot_r.at[i],
            device_id={"kv": kv + 1 + near + i, "tp": t}, device_id_type=MESH)

    def name_send(i, _):
        name_copy(i).start()
        return 0

    def near_send(i, _):
        near_copy(i).start()
        return 0

    lax.fori_loop(0, names_out, name_send, 0)

    l_in.wait()
    l_out.wait()
    cos_o, sin_o = outer[0:1, :], outer[1:2, :]
    cos_i, sin_i = inner[0], inner[1]
    cosine = cos_o * cos_i - sin_o * sin_i
    sine = sin_o * cos_i + cos_o * sin_i
    lane = iota((rows, LANES), 1)
    low = lane < HEAD_DIM
    first = lane % HEAD_DIM < HEAD_DIM // 2
    quarter = HEAD_DIM // 2

    def rotate(x):
        other = jnp.where(first, pltpu.roll(x, LANES - quarter, 1), pltpu.roll(x, quarter, 1))
        return x * cosine + other * sine

    l_tok.wait()
    l_wk.wait()
    l_wv.wait()
    both = dot(tok[...], wkv[...])
    keys = rotate(both[:, 0:LANES])
    values = both[:, LANES:]
    kv_all[0] = jnp.where(low, keys, swap(values))
    kv_all[1] = jnp.where(low, swap(keys), values)
    kv_own[...] = kv_all[tp].astype(BF16)

    lax.fori_loop(0, after_near, near_send, 0)
    l_wq.wait()
    queries = dot(tok[...], wq[...])
    main = rows // LANES
    tail = rows % LANES
    kinds = [m for m in range(main) for _ in range(2)] + [main] * (tail > 0)
    per = len(kinds)
    for p in range(heads // 2):
        turned = rotate(queries[:, p * LANES:(p + 1) * LANES])
        flat = jnp.transpose(turned[0:main * LANES])
        for m in range(main):
            for e in range(2):
                at = (p * per + 2 * m + e) * LANES
                part = flat[e * HEAD_DIM:(e + 1) * HEAD_DIM, m * LANES:(m + 1) * LANES]
                q_all[:, at:at + LANES] = part.astype(BF16)
        if tail:
            rest = turned[main * LANES:]
            both = jnp.transpose(jnp.concatenate([rest, swap(rest)], axis=0))
            at = (p * per + per - 1) * LANES
            q_all[:, at:at + LANES] = both[0:HEAD_DIM].astype(BF16)

    l_doc.wait()
    lane_row = iota((1, LANES), 1)
    wide_row = iota((8, LANES), 1)
    q_row = [m * LANES + lane_row for m in range(main)] + [main * LANES + lane_row % SPAN] * (tail > 0)
    wide_q = [m * LANES + wide_row for m in range(main)] + [main * LANES + wide_row % SPAN] * (tail > 0)
    q_pos = [kv * rows + row for row in q_row]
    q_start = [jnp.zeros((1, LANES), jnp.int32) for _ in q_row]
    end = jnp.int32(0)
    for i in range(doc.shape[1]):
        end = end + doc[0, i]
        q_start = [jnp.where(pos >= end, end, s) for pos, s in zip(q_pos, q_start)]
    place = iota((BLOCK, LANES), 0)

    def set_bias(key_block, count, causal):
        found = []
        for b in range(blocks):
            same = slot_rows[b] == key_block[:, 0:slot_rows[b].shape[1]]
            found.append(jnp.max(jnp.where(same, 1.0, 0.0), axis=1, keepdims=True))
        for r in range(len(q_row)):
            begin = r * LANES // BLOCK
            stop = min(begin + LANES // BLOCK, blocks)
            named = found[begin]
            for b in range(begin + 1, stop):
                named = jnp.where(wide_q[r] >= b * BLOCK, found[b], named)
            floor = jnp.where(named > 0.5, q_start[r] - key_block * BLOCK, FAR_OFF)
            for k in range(count):
                live = place >= floor[k:k + 1, :]
                if causal:
                    live = live & (place <= q_pos[r] - (kv * rows + k * BLOCK))
                bias[k * BLOCK:(k + 1) * BLOCK, r * LANES:(r + 1) * LANES] = jnp.where(live, 0.0, -jnp.inf)

    def set_values(block):
        count = block.shape[0]
        vt[0:HEAD_DIM, 0:count] = jnp.transpose(block)[HEAD_DIM:, :]

    def score(c, block):
        return dot(block[:, 0:HEAD_DIM], q_all[:, c * CHUNK:(c + 1) * CHUNK])

    def absorb(c, scores, fresh):
        count = scores.shape[0]
        cut = slice(c * CHUNK, (c + 1) * CHUNK)
        tiles = []
        for t in range(CHUNK // LANES):
            r = kinds[(c * (CHUNK // LANES) + t) % per]
            tiles.append(scores[:, t * LANES:(t + 1) * LANES] + bias[0:count, r * LANES:(r + 1) * LANES])
        scores = jnp.concatenate(tiles, axis=1)
        highest = jnp.max(scores, axis=0, keepdims=True)
        if not fresh:
            old = top[:, cut]
            highest = jnp.maximum(highest, old)
        weights = jnp.exp2((scores - highest) * SCALE).astype(BF16)
        summed = dot(vt[:, 0:count], weights)
        if not fresh:
            summed = summed + acc[:, cut] * jnp.exp2((old - highest) * SCALE)
        acc[:, cut] = summed
        top[:, cut] = highest

    def attend(begin, stop, block, fresh, after=None):
        ready = [score(c, block) for c in range(begin, min(begin + DEPTH, stop))]
        for c in range(begin, stop):
            now = ready.pop(0)
            if c + DEPTH < stop:
                ready.append(score(c + DEPTH, block))
            absorb(c, now, fresh)
            if after is not None:
                after(c)

    chunks = heads * rows // CHUNK
    vt[HEAD_DIM:, :] = jnp.ones((vt.shape[0] - HEAD_DIM, vt.shape[1]), BF16)
    local_block = iota((8, LANES), 0)
    set_bias(jnp.where(local_block < blocks, kv * blocks + local_block, -2), blocks, True)
    set_values(kv_own[...])
    def choose(flag):
        rank = jnp.zeros((1, LANES), F32)
        weight = [[], []]
        label = [jnp.zeros((1, LANES), F32) for _ in range(HOT)]
        for b in range(blocks):
            for s in range(HOT):
                one = jnp.where((flag[b] > 0.5) & (rank == s), 1.0, 0.0)
                weight[s].append(one)
                label[s] = label[s] + one * (b + 1)
            rank = rank + flag[b]
        return weight, label

    def gather(weight, block):
        total = block(0) * weight[0]
        for b in range(1, blocks):
            total = total + block(b) * weight[b]
        return total

    def choose_from(flags):
        return choose([flags[b:b + 1, :] for b in range(blocks)])

    def hot_send(i, _):
        name_copy(i).wait_recv()
        weight, _ = choose_from(names_in[i])
        for t in range(2):
            for s in range(HOT):
                part = gather(weight[s], lambda b: kv_all[t, b * BLOCK:(b + 1) * BLOCK, :])
                pack[i, t, s * BLOCK:(s + 1) * BLOCK, :] = part.astype(BF16)
            hot_copy(i, t).start()
        return 0

    ahead = kv % 2 == 1
    lax.fori_loop(0, jnp.where(ahead, 0, hots_out), hot_send, 0)

    own = kv_own[...]
    attend(0, chunks, own, True)
    lax.fori_loop(0, jnp.where(ahead, jnp.minimum(hots_out, 1), 0), hot_send, 0)

    def near_wait(i, _):
        near_copy(i).wait_recv()
        return 0

    def key_blocks(labels):
        found = [jnp.where(v > 0.5, base + v.astype(jnp.int32) - 1, -2) for base, v in labels]
        found += [jnp.full((1, LANES), -2, jnp.int32)] * (8 - len(found))
        return jnp.concatenate(found, axis=0)

    chosen = [choose_from(names[i]) for i in range(near)]
    set_bias(key_blocks([((kv - 1 - i) * blocks, v) for i in range(near) for v in chosen[i][1]]), near * HOT, False)
    lax.fori_loop(0, before_near, near_wait, 0)
    for i in range(near):
        for s in range(HOT):
            part = gather(chosen[i][0][s], lambda b: near_in[i, b * BLOCK:(b + 1) * BLOCK, :].astype(F32))
            at = (i * HOT + s) * BLOCK
            near_keys[at:at + BLOCK, :] = part.astype(BF16)
    block = near_keys[...]
    set_values(block)
    attend(0, chunks, block, False)

    lax.fori_loop(1, jnp.where(ahead, hots_out, 1), hot_send, 0)

    def att_copy(h):
        return pltpu.make_async_remote_copy(
            src_ref=att.at[h], dst_ref=att_in.at[h], send_sem=att_s.at[h], recv_sem=att_r.at[h],
            device_id={"tp": 1 - tp}, device_id_type=MESH)

    def hot_wait(i, _):
        hot_copy(i, tp).wait_recv()
        return 0


    def far_bias(start):
        labels = []
        for i in range(STEP):
            _, label = choose_from(names[near + start + i])
            labels += [((kv - 1 - near - start - i) * blocks, v) for v in label]
        set_bias(key_blocks(labels), STEP * HOT, False)

    def far_block(start):
        block = hot_in[pl.ds(start, STEP)].reshape(STEP * kept, LANES)
        set_values(block)
        return block

    steps = far // STEP
    if steps > 1:
        lax.fori_loop(0, before_far, hot_wait, 0)

        def far_step(g, _):
            far_bias(g * STEP)
            block = far_block(g * STEP)
            attend(0, chunks, block, False)
            return 0

        lax.fori_loop(0, steps - 1, far_step, 0)
    far_bias((steps - 1) * STEP)
    if steps == 1:
        lax.fori_loop(0, before_far, hot_wait, 0)
    block = far_block((steps - 1) * STEP)
    low_tile = iota((SPAN, LANES), 1) < HEAD_DIM

    def finish_half(h):
        for p in range(h * heads // 2 // halves, (h + 1) * heads // 2 // halves):
            at = p * LANES - h * width

            def scaled(t):
                cut = slice((p * per + t) * LANES, (p * per + t + 1) * LANES)
                return (acc[0:HEAD_DIM, cut] * (1.0 / acc[HEAD_DIM:HEAD_DIM + 1, cut])).astype(BF16)

            for m in range(main):
                part = jnp.transpose(jnp.concatenate([scaled(2 * m), scaled(2 * m + 1)], axis=0))
                att[h, m * LANES:(m + 1) * LANES, at:at + LANES] = part
            if tail:
                part = scaled(per - 1)
                turned = jnp.transpose(jnp.concatenate([part, part], axis=0))
                part = jnp.where(low_tile, turned[0:SPAN], turned[SPAN:])
                att[h, main * LANES:, at:at + LANES] = part
        att_copy(h).start()

    some = chunks // halves
    ready = [score(c, block) for c in range(some)]
    for h in range(halves):
        now = ready
        for c in range(some):
            absorb(h * some + c, now[c], False)
        if h + 1 < halves:
            ready = [score((h + 1) * some + c, block) for c in range(some)]
        finish_half(h)

    l_wo0.wait()
    columns = wo.shape[1]
    piece = columns // 4
    for c in range(4):
        cut = slice(c * piece, (c + 1) * piece)
        value = dot(att[0], wo[0:width, cut])
        for h in range(1, halves):
            value += dot(att[h], wo[h * width:(h + 1) * width, cut])
        partial[:, cut] = value
    l_wo1.wait()
    att_copy(0).wait_recv()
    for h in range(halves - 1):
        if h:
            att_copy(h).wait_recv()
        for c in range(4):
            cut = slice(c * piece, (c + 1) * piece)
            partial[:, cut] += dot(att_in[h], wo[mine + h * width:mine + (h + 1) * width, cut])
    att_copy(halves - 1).wait_recv()
    last[...] = att_in[halves - 1]
    l_wo2.wait()

    def name_done(i, _):
        name_copy(i).wait_send()
        return 0

    def near_done(i, _):
        near_copy(i).wait_send()
        return 0

    def hot_done(i, _):
        for t in range(2):
            hot_copy(i, t).wait_send()
        return 0

    lax.fori_loop(0, names_out, name_done, 0)
    lax.fori_loop(0, after_near, near_done, 0)
    lax.fori_loop(0, hots_out, hot_done, 0)
    for h in range(halves):
        att_copy(h).wait_send()


def finish(partial, last, weight, out, stage, sem):
    pieces = stage.shape[0]
    wide = stage.shape[2]
    cuts = [slice(c * wide, (c + 1) * wide) for c in range(pieces)]
    stores = [pltpu.make_async_copy(stage.at[c], out.at[0, :, cuts[c]], sem.at[c]) for c in range(pieces)]
    ready = dot(last[...], weight[:, cuts[0]])
    for c in range(pieces):
        stage[c] = (partial[:, cuts[c]] + ready).astype(BF16)
        if c + 1 < pieces:
            ready = dot(last[...], weight[:, cuts[c + 1]])
        stores[c].start()
    for store in stores:
        store.wait()


def solution(mesh):
    n = mesh.shape["kv"]

    def shards(tokens, doc_lengths, picked, w_query, w_key, w_value, w_out):
        _, rows, d = tokens.shape
        blocks = rows // BLOCK
        pad = -(-blocks // 8) * 8
        q_cols = w_query.shape[1]
        heads = q_cols // HEAD_DIM
        columns = w_out.shape[1]
        inner, outer = tables(rows, n)
        width = q_cols // 2
        dma = pltpu.SemaphoreType.DMA
        payload = HOT * BLOCK
        reach = min(n, (n * rows // 2 + rows - 2) // rows)
        near = NEAR
        far = -(-max(reach - near, 1) // STEP) * STEP
        most = max(rows, near * payload, STEP * payload)
        operands = (tokens, doc_lengths, jnp.transpose(picked, (1, 0, 2)), w_query, w_key, w_value, w_out, inner, outer)
        operands = [pltpu.with_memory_space_constraint(jnp.asarray(x), pltpu.HBM) for x in operands]
        vmem = pl.BlockSpec(memory_space=pltpu.VMEM)
        parts = pl.pallas_call(
            functools.partial(kernel, n, near, far),
            out_shape=[
                jax.ShapeDtypeStruct((rows, columns), F32),
                jax.ShapeDtypeStruct((rows, width), BF16),
                jax.ShapeDtypeStruct((width, columns), BF16),
            ],
            in_specs=[pl.BlockSpec(memory_space=pltpu.HBM)] * 9,
            out_specs=[vmem] * 3,
            scratch_shapes=[
                pltpu.VMEM((rows, d), BF16),
                pltpu.SMEM(doc_lengths.shape, jnp.int32),
                pltpu.VMEM((blocks, 1, picked.shape[2]), jnp.int32),
                pltpu.VMEM(w_query.shape, BF16),
                pltpu.VMEM((d, 2 * LANES), BF16),
                pltpu.VMEM((w_out.shape[0] - width, columns), BF16),
                pltpu.VMEM(inner.shape, F32),
                pltpu.VMEM(outer.shape[1:], F32),
                pltpu.VMEM((near + far, pad, LANES), F32),
                pltpu.VMEM((far, pad, LANES), F32),
                pltpu.VMEM((2, rows, LANES), F32),
                pltpu.VMEM((rows, LANES), BF16),
                pltpu.VMEM((near, rows, LANES), BF16),
                pltpu.VMEM((near * payload, LANES), BF16),
                pltpu.VMEM((far, 2, payload, LANES), BF16),
                pltpu.VMEM((far, payload, LANES), BF16),
                pltpu.VMEM((most, -(-rows // LANES) * LANES), F32),
                pltpu.VMEM((HEAD_DIM + 16, most), BF16),
                pltpu.VMEM((HEAD_DIM, heads * rows), BF16),
                pltpu.VMEM((HEAD_DIM + 16, heads * rows), F32),
                pltpu.VMEM((1, heads * rows), F32),
                pltpu.VMEM((2, rows, width), BF16),
                pltpu.VMEM((2, rows, width), BF16),
                dma((11,)), dma((far,)), dma((far,)), dma((near,)), dma((near,)),
                dma((far, 2)), dma((far,)), dma((2,)), dma((2,)),
            ],
            compiler_params=pltpu.CompilerParams(
                collective_id=0, has_side_effects=True, vmem_limit_bytes=28 * 1024 * 1024
            ),
        )(*operands)
        return pl.pallas_call(
            finish,
            out_shape=jax.ShapeDtypeStruct((1, rows, columns), BF16),
            in_specs=[vmem] * 3,
            out_specs=pl.BlockSpec(memory_space=pltpu.HBM),
            scratch_shapes=[pltpu.VMEM((PIECES, rows, columns // PIECES), BF16), dma((PIECES,))],
            compiler_params=pltpu.CompilerParams(vmem_limit_bytes=8 * 1024 * 1024),
        )(*parts)

    placed = (P("dp", "kv", None), P("dp", None), P("dp", "kv", None), P(None, "tp"), P(), P(), P())
    return jax.shard_map(
        shards, mesh=mesh, in_specs=placed, out_specs=P("dp", "kv", None), check_vma=False
    )
```
